512 devices in a mesh: ep: 128 (over z, x, core), tp: 4 (over y).
Axes of the slice: x: 4, y: 4, z: 16, core: 2. Of those that a mesh axis runs over, the one named last changes fastest.
Arguments:
- tokens: bfloat16 [1664, 1024], P('ep'), may hold values from -60 to 60
- attn_gain: float32 [1024], replicated, may hold values from 0.1 to 1.9
- query_weight: bfloat16 [1024, 512], P(None, 'tp'), may hold values from -0.1875 to 0.1875
- key_weight: bfloat16 [1024, 256], P(None, 'tp'), may hold values from -0.1875 to 0.1875
- value_weight: bfloat16 [1024, 256], P(None, 'tp'), may hold values from -0.1875 to 0.1875
- forget_weight: bfloat16 [1024, 8], P(None, 'tp'), may hold values from -0.5 to 0.5
- forget_bias: float32 [8], P('tp'), may hold values from -3 to 3
- out_weight: bfloat16 [512, 1024], P('tp'), may hold values from -0.75 to 0.75
- key_cache: bfloat16 [1664, 4, 64, 1024], P('ep', 'tp'), may hold values from -300 to 300
- value_cache: bfloat16 [1664, 4, 64, 1024], P('ep', 'tp'), may hold values from -12 to 12
- cum_forget: float32 [1664, 8, 1024], P('ep', 'tp'), may hold values from -131 to 0, as said below
- lengths: int32 [1664], P('ep'), may hold values from 256 to 1024
- ffn_gain: float32 [1024], replicated, may hold values from 0.1 to 1.9
- routes: int32 [1664, 2], P('ep'), may hold values from 0 to 31, all different within a row; in each aligned block of 13 rows (0 to 12, 13 to 25, ...) at most 2 rows name the same one
- route_weights: float32 [1664, 2], P('ep'), may hold values from 0.2 to 1
- gate_weight: bfloat16 [128, 1024, 512], P('ep', None, 'tp'), may hold values from -0.1875 to 0.1875
- up_weight: bfloat16 [128, 1024, 512], P('ep', None, 'tp'), may hold values from -0.1875 to 0.1875
- down_weight: bfloat16 [128, 512, 1024], P('ep', 'tp'), may hold values from -0.25 to 0.25
Outputs:
- layer_out: bfloat16 [1664, 1024], P('ep', 'tp')
The draws below stay inside these ranges and needn't reach their ends.
Inputs may be any that keep to these rules, and one draw needn't show every extreme that they name: `routes`: the experts of a row differ; in each aligned block of 13 rows (the rows of one index of ep) no expert is named by more than 2 rows. `cum_forget`: for each sequence and head the entries do not increase along positions.
All inputs are finite; a program needn't handle non-finite values.
Results may differ from the reference program's by a relative error of at most 0.0085.
Values may be sent and summed in bfloat16 or wider, within the bound.
No kernel may reach another device: no remote copies, remote signals or barrier semaphores. Data moves between devices by JAX's collectives and lax.ppermute only.
A program may use at most 64 MiB of HBM per device.

```python
import math
import jax
import jax.numpy as jnp
import numpy as np
from jax import lax

D = 1024
HEADS = 8
KVH = 4
HD = 64
FF = 2048
SLICES = 4
TOP_K = 2
SEQ_DEV = 13
STORED_SPAN = 1024
STREAM_TOTAL = 1664
EXPERTS = 32
CAP = 2
N_EP = 128
N_TP = 4


def draw_tokens(key, part):
    base_key, row_key = jax.random.split(key, 2)
    column = jnp.arange(D, dtype=jnp.float32) / (D - 1)
    values = jax.random.normal(base_key, (STREAM_TOTAL, D), jnp.float32)
    values = values * jnp.exp(jnp.log(10.0) * column)[None, :]
    row_scale = jnp.exp(jax.random.uniform(row_key, (STREAM_TOTAL, 1), jnp.float32, jnp.log(0.5), jnp.log(2.0)))
    return jnp.clip(values * row_scale, -60.0, 60.0).astype(jnp.bfloat16)


def draw_key_cache(key, part):
    noise_key = jax.random.fold_in(key, 0)
    shape = (STREAM_TOTAL, KVH, HD, STORED_SPAN)
    base = jax.random.normal(noise_key, shape, jnp.float32)
    return jnp.clip(base, -300.0, 300.0).astype(jnp.bfloat16)


def draw_value_cache(key, part):
    noise_key, level_key = jax.random.split(key, 2)
    blocks = STORED_SPAN // 64
    levels = jax.random.normal(level_key, (STREAM_TOTAL, KVH, HD, blocks, 1), jnp.float32)
    noise = jax.random.normal(noise_key, (STREAM_TOTAL, KVH, HD, blocks, 64), jnp.float32)
    return jnp.clip((noise + levels).reshape(STREAM_TOTAL, KVH, HD, STORED_SPAN), -12.0, 12.0).astype(jnp.bfloat16)


def draw_cum_forget(key, part):
    category_noise_seed, gradual_noise_seed, quick_noise_seed, stream_noise_seed, decoding_noise_seed, spike_noise_seed, layering_noise_seed = jax.random.split(key, 7)
    chance = 0.5
    fast = jax.random.uniform(category_noise_seed, (1, HEADS, 1), jnp.float32) < chance
    slow_rate = jax.random.uniform(gradual_noise_seed, (1, HEADS, 1), jnp.float32, 0.2, 0.6) / STORED_SPAN
    fast_rate = jax.random.uniform(quick_noise_seed, (1, HEADS, 1), jnp.float32, 1.0 / 50.0, 1.0 / 30.0)
    rate = jnp.where(fast, fast_rate, slow_rate)
    factor = jnp.exp(jax.random.uniform(stream_noise_seed, (STREAM_TOTAL, 1, 1), jnp.float32, jnp.log(0.5), jnp.log(2.0)))
    rough = jax.random.uniform(decoding_noise_seed, (STREAM_TOTAL, HEADS, STORED_SPAN), jnp.float32, 0.5, 1.5)
    stored_offsets = jax.random.randint(spike_noise_seed, (STREAM_TOTAL, 1, 2), 0, STORED_SPAN)
    position = lax.broadcasted_iota(jnp.int32, (1, 1, STORED_SPAN, 1), 2)
    hits = jnp.sum((position == stored_offsets[:, :, None, :]).astype(jnp.float32), axis=3)
    depth = jax.random.uniform(layering_noise_seed, (STREAM_TOTAL, HEADS, 1), jnp.float32, 0.22, 0.5)
    steps = -rate * factor * rough - hits * depth
    return jnp.clip(jnp.cumsum(steps, axis=2), -(STORED_SPAN // 8) - 3.0, 0.0)


def touch_ends(array, stream_key, low, largest):
    shape = array.shape
    spot = [jax.random.randint(jax.random.fold_in(stream_key, axis), (), 0, shape[axis]) for axis in range(len(shape))]
    array = array.at[tuple(spot)].set(low)
    longest = shape.index(max(shape))
    spot[longest] = (spot[longest] + 1) % shape[longest]
    return array.at[tuple(spot)].set(largest)


def block_scale(rng, shape, shards, low, top_value):
    loudness = 1.0
    for dim, blocks in shards:
        heights = jax.random.uniform(jax.random.fold_in(jax.random.fold_in(rng, 6), dim), (blocks,), jnp.float32, low / len(shards), top_value / len(shards))
        loudness = loudness * jnp.repeat(jnp.exp(heights), shape[dim] // blocks).reshape((-1,) + (1,) * (len(shape) - 1 - dim))
    return loudness


def assign_block(rng, own, number, rows, number_of, top, limit, slope):
    order = jax.random.permutation(rng, number_of)
    heavy_load, common = portions_of(number_of, rows * top, limit, slope, True), portions_of(number_of, rows * top, limit, slope, False)
    places = jnp.arange(number_of)

    def named(tallies, turn):
        used = int((tallies > 0).sum())
        fixed = max(1, used // 4)
        moved = fixed + (places - fixed + turn * (used - fixed)) % max(1, number_of - fixed)
        return jnp.zeros((number_of,), jnp.int32).at[order[jnp.where(places < fixed, places, moved)]].set(jnp.asarray(tallies, jnp.int32))

    tallies = jnp.where(number % 4 == 0, named(heavy_load, number // 4), named(common, number - number // 4 - 1))
    mixed = jax.random.permutation(jax.random.fold_in(own, 3), number_of)
    donor, receiver = mixed[0:number_of // 2 * 2:2], mixed[1:number_of // 2 * 2:2]
    margin = jnp.minimum(tallies[donor] - 1, limit - tallies[receiver]) // 2
    margin = jnp.where((donor == order[0]) | (receiver == order[0]) | (tallies[receiver] == 0), 0, jnp.maximum(margin, 0))
    moved = jax.random.randint(jax.random.fold_in(own, 4), (number_of // 2,), 0, 1 << 20) % (margin + 1)
    tallies = tallies.at[donor].add(-moved).at[receiver].add(moved)
    members = jnp.searchsorted(jnp.cumsum(tallies), jnp.arange(rows * top), side="right").astype(jnp.int32)
    table = members.reshape(top, rows).T
    table = table[jax.random.permutation(jax.random.fold_in(own, 1), rows)]
    turn = jax.random.randint(jax.random.fold_in(own, 2), (rows, 1), 0, top)
    return jnp.take_along_axis(table, (jnp.arange(top)[None, :] + turn) % top, axis=1)


def portions_of(amount, total, limit, slope, full):
    weights = [(1 << 20) // math.isqrt(standing ** slope) + 1 for standing in range(1, amount + 1)]
    largest = limit if full else min(limit, max(-(-total // amount), total * weights[0] // sum(weights)))
    least = 1 if total - largest >= amount - 1 else 0
    holding, surplus = [largest] + [least] * (amount - 1), total - largest - least * (amount - 1)
    while surplus > 0:
        movable = [i for i in range(1, amount) if holding[i] < largest] or [i for i in range(1, amount) if holding[i] < limit]
        pool, budget = sum([weights[i] for i in movable]), surplus
        for i in movable:
            addition = min(limit - holding[i], max(1, budget * weights[i] // pool), surplus)
            holding[i] = holding[i] + addition
            surplus = surplus - addition
    return np.array(holding)


def scatter_about(stream_key, dims, spread, reach, shards=(), kind=jnp.bfloat16):
    array = spread * jax.random.normal(stream_key, dims, jnp.float32)
    if shards:
        array = array * block_scale(stream_key, dims, shards, -0.22, 0.18)
    return jnp.clip(array, -reach, reach).astype(kind)


def setup_inputs(seed: int = 0) -> dict:
    streams_of = jax.random.split(jax.random.key(seed), 19)
    tokens = draw_tokens(jax.random.fold_in(streams_of[18], 71), 0)
    attn_gain = jnp.clip(1.0 + 0.18 * jax.random.normal(streams_of[1], (D,), jnp.float32), 0.1, 1.9)
    query_weight = scatter_about(streams_of[2], (D, HEADS * HD), D ** -0.5, 0.1875, ((1, 4),))
    key_weight = scatter_about(streams_of[3], (D, KVH * HD), D ** -0.5, 0.1875, ((1, 4),))
    value_weight = scatter_about(streams_of[4], (D, KVH * HD), D ** -0.5, 0.1875, ((1, 4),))
    forget_weight = scatter_about(streams_of[5], (D, HEADS), (D // 9) ** -0.5, 0.5, ((1, 4),))
    forget_bias = jnp.clip(jax.random.uniform(streams_of[6], (HEADS,), jnp.float32, -3.0, 3.0) * block_scale(streams_of[6], (HEADS,), ((0, 4),), -0.4, 0.0), -3.0, 3.0)
    out_weight = scatter_about(streams_of[7], (HEADS * HD, D), (HEADS * HD // 8) ** -0.5, 0.75, ((0, 4),))
    key_cache = draw_key_cache(jax.random.fold_in(streams_of[18], 71), 0)
    value_cache = draw_value_cache(jax.random.fold_in(streams_of[18], 71), 0)
    cum_forget = draw_cum_forget(jax.random.fold_in(streams_of[18], 71), 0)
    lengths = touch_ends(jax.random.randint(streams_of[11], (STREAM_TOTAL,), STORED_SPAN // 4, STORED_SPAN + 1), jax.random.fold_in(streams_of[11], 1), STORED_SPAN // 4, STORED_SPAN).astype(jnp.int32)
    ffn_gain = jnp.clip(1.0 + 0.18 * jax.random.normal(streams_of[12], (D,), jnp.float32), 0.1, 1.9)
    routes_keys = jax.random.split(jax.random.fold_in(streams_of[13], 1), STREAM_TOTAL // SEQ_DEV)
    routes_turns = jax.random.permutation(jax.random.fold_in(streams_of[13], 3), STREAM_TOTAL // SEQ_DEV)
    routes = jax.vmap(lambda own, number: assign_block(jax.random.fold_in(streams_of[13], 2), own, number, SEQ_DEV, EXPERTS, TOP_K, CAP, 1))(routes_keys, routes_turns).reshape((STREAM_TOTAL, TOP_K))
    route_weights = jnp.clip(0.2 + 0.8 * jax.random.uniform(streams_of[14], (STREAM_TOTAL, TOP_K), jnp.float32) ** block_scale(streams_of[14], (STREAM_TOTAL, TOP_K), ((0, 128),), -0.2, 0.2), 0.2, 1.0)
    gate_weight = scatter_about(streams_of[15], (EXPERTS * SLICES, D, FF // SLICES), D ** -0.5, 0.1875, ((0, 128), (2, 4)))
    up_weight = scatter_about(streams_of[16], (EXPERTS * SLICES, D, FF // SLICES), D ** -0.5, 0.1875, ((0, 128), (2, 4)))
    down_weight = scatter_about(streams_of[17], (EXPERTS * SLICES, FF // SLICES, D), (FF // 4) ** -0.5, 0.25, ((0, 128), (1, 4)))
    return {"tokens": tokens, "attn_gain": attn_gain, "query_weight": query_weight, "key_weight": key_weight, "value_weight": value_weight, "forget_weight": forget_weight, "forget_bias": forget_bias, "out_weight": out_weight, "key_cache": key_cache, "value_cache": value_cache, "cum_forget": cum_forget, "lengths": lengths, "ffn_gain": ffn_gain, "routes": routes, "route_weights": route_weights, "gate_weight": gate_weight, "up_weight": up_weight, "down_weight": down_weight}


EPSILON = 1e-06

def round_trip(values):
    return lax.optimization_barrier(values.astype(jnp.bfloat16)).astype(jnp.float32)

def normalize(values, gain):
    return values * lax.rsqrt(lax.optimization_barrier(jnp.mean(values * values, axis=-1, keepdims=True)) + EPSILON) * gain

def block_slots(group_routes):
    assigned = group_routes.reshape(-1).astype(jnp.int32)
    member = (assigned[:, None] == jnp.arange(EXPERTS, dtype=jnp.int32)[None, :]).astype(jnp.int32)
    earlier = (jnp.cumsum(member, axis=0) - member).astype(jnp.int32)
    return (assigned * CAP + lax.optimization_barrier(jnp.sum(earlier * member, axis=1))).astype(jnp.int32)

def reference(tokens, attn_gain, query_weight, key_weight, value_weight, forget_weight, forget_bias, out_weight, key_cache, value_cache, cum_forget, lengths, ffn_gain, routes, route_weights, gate_weight, up_weight, down_weight):
    group = HEADS // KVH
    score_scale = HD ** (-0.5)
    token_f = tokens.astype(jnp.float32)
    normed = normalize(token_f, attn_gain).astype(jnp.bfloat16)

    def attend(pack):
        normed_rows, keys, values, cumul, lens = pack
        count = normed_rows.shape[0]
        query_rows = jnp.dot(normed_rows, query_weight, preferred_element_type=jnp.float32).astype(jnp.bfloat16)
        query_rows = query_rows.reshape(count, KVH, group, HD).astype(jnp.float32)
        fresh_keys = jnp.dot(normed_rows, key_weight, preferred_element_type=jnp.float32).astype(jnp.bfloat16)
        fresh_keys = fresh_keys.reshape(count, KVH, HD).astype(jnp.float32)
        new_values = jnp.dot(normed_rows, value_weight, preferred_element_type=jnp.float32).astype(jnp.bfloat16)
        new_values = new_values.reshape(count, KVH, HD).astype(jnp.float32)
        log_forget = jax.nn.log_sigmoid(jnp.dot(normed_rows, forget_weight, preferred_element_type=jnp.float32) + forget_bias)
        log_forget = log_forget.reshape(count, KVH, group)
        scores = jnp.einsum('bkgd,bkdl->bkgl', query_rows, keys.astype(jnp.float32)) * score_scale
        cumul = cumul.reshape(count, KVH, group, STORED_SPAN)
        last_index = jnp.broadcast_to((lens - 1).astype(jnp.int32)[:, None, None, None], (count, KVH, group, 1))
        last = jnp.take_along_axis(cumul, last_index, axis=3)
        positions = jnp.arange(STORED_SPAN, dtype=jnp.int32)[None, None, None, :]
        valid = positions < lens[:, None, None, None]
        scores = jnp.where(valid, scores + (last - cumul) + log_forget[..., None], -jnp.inf)
        self_score = jnp.einsum('qvml,qvl->qvm', query_rows, fresh_keys) * score_scale
        top = jnp.maximum(lax.optimization_barrier(jnp.max(scores, axis=3)), self_score)
        expo = jnp.exp(scores - top[..., None])
        own_exp = jnp.exp(self_score - top)
        total = lax.optimization_barrier(jnp.sum(expo, axis=3)) + own_exp
        weights = round_trip(expo / total[..., None])
        own_weight = round_trip(own_exp / total)
        mixed_heads = jnp.einsum('bkgl,bkdl->bkgd', weights, values.astype(jnp.float32))
        mixed_heads = mixed_heads + own_weight[..., None] * new_values[:, :, None, :]
        heads_out = round_trip(mixed_heads).reshape(count, N_TP, HEADS * HD // N_TP)
        blocks = out_weight.reshape(N_TP, HEADS * HD // N_TP, D).astype(jnp.float32)
        partial_value = jnp.einsum('bnc,ncd->nbd', heads_out, blocks)
        return lax.optimization_barrier(jnp.sum(round_trip(partial_value), axis=0))
    mixed = lax.map(attend, (normed.reshape(N_EP, SEQ_DEV, D), key_cache.reshape(N_EP, SEQ_DEV, KVH, HD, STORED_SPAN), value_cache.reshape(N_EP, SEQ_DEV, KVH, HD, STORED_SPAN), cum_forget.reshape(N_EP, SEQ_DEV, HEADS, STORED_SPAN), lengths.reshape(N_EP, SEQ_DEV))).reshape(STREAM_TOTAL, D)
    residual = round_trip(token_f + mixed)
    ffn_in = normalize(residual, ffn_gain).astype(jnp.bfloat16)
    slots = jax.vmap(block_slots)(routes.reshape(N_EP, SEQ_DEV, TOP_K))
    slot_expert = (slots // CAP).astype(jnp.int32)
    slot_index = (slots % CAP).astype(jnp.int32)
    spread_rows = jnp.repeat(ffn_in.reshape(N_EP, SEQ_DEV, D), TOP_K, axis=1).astype(jnp.float32)
    flat_weights = route_weights.reshape(N_EP, SEQ_DEV * TOP_K)
    units = FF // SLICES
    part_units = units // N_TP
    capacity_iota = jnp.arange(CAP, dtype=jnp.int32)

    def per_expert(routed, pack):
        expert, gates, ups, downs = pack
        chosen = slot_expert == expert
        place = (chosen[:, None, :] & (slot_index[:, None, :] == capacity_iota[None, :, None])).astype(jnp.float32)
        expert_rows = jnp.einsum('gca,gad->gcd', place, spread_rows, precision=lax.Precision.HIGHEST)
        expert_rows = expert_rows.astype(jnp.bfloat16).reshape(N_EP * CAP, D)

        def one_slice(total, weights):
            gate_w, up_w, down_w = weights
            gate = jnp.dot(expert_rows, gate_w, preferred_element_type=jnp.float32)
            up = jnp.dot(expert_rows, up_w, preferred_element_type=jnp.float32)
            hidden = round_trip(jax.nn.silu(gate) * up).reshape(N_EP * CAP, N_TP, part_units)
            parts = jnp.einsum('rnu,nud->nrd', hidden, down_w.reshape(N_TP, part_units, D).astype(jnp.float32))
            return (total + round_trip(lax.optimization_barrier(jnp.sum(round_trip(parts), axis=0))), None)
        served, _ = lax.scan(one_slice, jnp.zeros((N_EP * CAP, D), jnp.float32), (gates, ups, downs))
        picked = jnp.einsum('gca,gcd->gad', place, served.reshape(N_EP, CAP, D), precision=lax.Precision.HIGHEST)
        share = (flat_weights * chosen.astype(jnp.float32))[..., None] * picked
        return (routed + lax.optimization_barrier(jnp.sum(share.reshape(STREAM_TOTAL, TOP_K, D), axis=1)), None)
    routed, _ = lax.scan(per_expert, jnp.zeros((STREAM_TOTAL, D), jnp.float32), (jnp.arange(EXPERTS, dtype=jnp.int32), gate_weight.reshape(EXPERTS, SLICES, D, units), up_weight.reshape(EXPERTS, SLICES, D, units), down_weight.reshape(EXPERTS, SLICES, units, D)))
    return (residual + routed).astype(jnp.bfloat16)
```

```python
import jax
import jax.numpy as jnp
from jax import lax
from jax.sharding import Mesh
from jax.sharding import PartitionSpec as P

HEADS = 8
KVH = 4
HD = 64
SLICES = 4
TOP_K = 2
STORED_SPAN = 1024


EPSILON = 1e-06
EXPERT_AXES = ("z", "xh")
SLICE_AXES = ("xl", "core")
EP_AXES = EXPERT_AXES + SLICE_AXES
GROUP_AXES = SLICE_AXES + ("tp",)


def copy_for_each(shard, axis):
    copies = jnp.broadcast_to(shard, (lax.axis_size(axis), *shard.shape))
    return lax.all_to_all(copies, axis, split_axis=0, concat_axis=0, tiled=True)


def in_blocks(shard, dim, devices):
    before, after = (shard.shape[:dim], shard.shape[dim + 1 :])
    return jnp.moveaxis(shard.reshape(*before, devices, -1, *after), dim, 0)


def sent_and_summed(shard, axis, dim):
    devices = lax.axis_size(axis)
    blocks = lax.all_to_all(in_blocks(shard, dim, devices), axis, 0, 0, tiled=True)
    return jnp.sum(blocks.astype(jnp.float32), axis=0)


def round_trip(values):
    return lax.optimization_barrier(values.astype(jnp.bfloat16)).astype(jnp.float32)


def inverse_rms(values, width):
    return lax.rsqrt(jnp.sum(values * values, axis=-1, keepdims=True) / width + EPSILON)


def slot_tables(routes, route_weights, experts, capacity):
    seq_rows = routes.shape[0]
    expert = lax.broadcasted_iota(jnp.int32, (experts, 1, 1), 0)
    chosen = routes[None] == expert
    named = jnp.any(chosen, axis=2).astype(jnp.float32)
    share = jnp.sum(jnp.where(chosen, route_weights[None], 0.0), axis=2)
    first = lax.broadcasted_iota(jnp.int32, (seq_rows, seq_rows), 0)
    second = lax.broadcasted_iota(jnp.int32, (seq_rows, seq_rows), 1)
    earlier = jnp.dot(named, (first < second).astype(jnp.float32))
    slot = lax.broadcasted_iota(jnp.int32, (1, capacity, 1), 1).astype(jnp.float32)
    here = (earlier[:, None, :] == slot) & (named[:, None, :] > 0.0)
    place = here.astype(jnp.bfloat16).reshape(experts * capacity, seq_rows)
    weighted = jnp.where(here, share[:, None, :], 0.0).reshape(experts * capacity, seq_rows)
    return place, weighted.T


def body(
    tokens,
    attn_gain,
    query_weight,
    key_weight,
    value_weight,
    forget_weight,
    forget_bias,
    out_weight,
    key_cache,
    value_cache,
    cum_forget,
    lengths,
    ffn_gain,
    routes,
    route_weights,
    gate_weight,
    up_weight,
    down_weight,
):
    tp_count = lax.axis_size("tp")
    ep_count = lax.axis_size(EXPERT_AXES) * SLICES
    tp_rank = lax.axis_index("tp")
    seq_rows = tokens.shape[0]
    width = tokens.shape[1]
    cols = width // tp_count
    experts = ep_count // SLICES
    capacity = min(seq_rows, max(2, (2 * seq_rows * TOP_K + experts - 1) // experts))
    kv_local = key_cache.shape[1]
    group = HEADS // KVH
    score_scale = HD ** (-0.5)
    token_f = tokens.astype(jnp.float32)
    normed = (token_f * inverse_rms(token_f, width) * attn_gain).astype(jnp.bfloat16)
    query_rows = jnp.dot(normed, query_weight, preferred_element_type=jnp.float32).astype(
        jnp.bfloat16
    )
    query_rows = query_rows.reshape(seq_rows, kv_local, group, HD)
    fresh_keys = jnp.dot(normed, key_weight, preferred_element_type=jnp.float32).astype(
        jnp.bfloat16
    )
    fresh_keys = fresh_keys.reshape(seq_rows, kv_local, HD)
    new_values = jnp.dot(normed, value_weight, preferred_element_type=jnp.float32).astype(
        jnp.bfloat16
    )
    new_values = new_values.reshape(seq_rows, kv_local, HD)
    log_forget = jax.nn.log_sigmoid(
        jnp.dot(normed, forget_weight, preferred_element_type=jnp.float32) + forget_bias
    )
    log_forget = log_forget.reshape(seq_rows, kv_local, group)
    scores = (
        jnp.einsum("bkgd,bkdl->bkgl", query_rows, key_cache, preferred_element_type=jnp.float32)
        * score_scale
    )
    cumul = cum_forget.reshape(seq_rows, kv_local, group, STORED_SPAN)
    last_index = jnp.broadcast_to(
        (lengths - 1)[:, None, None, None], (seq_rows, kv_local, group, 1)
    )
    last = jnp.take_along_axis(cumul, last_index, axis=3)
    positions = lax.broadcasted_iota(jnp.int32, (1, 1, 1, STORED_SPAN), 3)
    valid = positions < lengths[:, None, None, None]
    scores = jnp.where(valid, scores + (last - cumul) + log_forget[..., None], -jnp.inf)
    self_score = (
        jnp.einsum("qvml,qvl->qvm", query_rows, fresh_keys, preferred_element_type=jnp.float32)
        * score_scale
    )
    top = jnp.maximum(jnp.max(scores, axis=3), self_score)
    expo = jnp.exp(scores - top[..., None])
    own_exp = jnp.exp(self_score - top)
    total = jnp.sum(expo, axis=3) + own_exp
    attn_weights = (expo / total[..., None]).astype(jnp.bfloat16)
    own_weight = round_trip(own_exp / total)
    heads_out = jnp.einsum(
        "bkgl,bkdl->bkgd", attn_weights, value_cache, preferred_element_type=jnp.float32
    )
    heads_out = heads_out + own_weight[..., None] * new_values.astype(jnp.float32)[:, :, None, :]
    heads_out = heads_out.astype(jnp.bfloat16).reshape(seq_rows, -1)
    partial_value = jnp.dot(heads_out, out_weight, preferred_element_type=jnp.float32)
    mixed_cols = sent_and_summed(partial_value.astype(jnp.bfloat16), "tp", 1)
    token_cols = lax.dynamic_slice_in_dim(token_f, tp_rank * cols, cols, 1)
    residual_cols = (token_cols + mixed_cols).astype(jnp.bfloat16)
    place, weighted = slot_tables(routes, route_weights, experts, capacity)
    outgoing = jnp.dot(place, residual_cols, preferred_element_type=jnp.float32)
    outgoing = outgoing.astype(jnp.bfloat16).reshape(experts, capacity, cols)
    arrived = lax.all_to_all(outgoing, EXPERT_AXES, split_axis=0, concat_axis=0, tiled=True)
    arrived = arrived.reshape(experts * capacity, cols)
    gathered = copy_for_each(arrived, GROUP_AXES)
    gathered = gathered.reshape(SLICES, tp_count, experts * capacity, cols)
    rows = jnp.transpose(gathered, (0, 2, 1, 3)).reshape(-1, width).astype(jnp.float32)
    flat = (rows * inverse_rms(rows, width) * ffn_gain).astype(jnp.bfloat16)
    gate = jnp.dot(flat, gate_weight[0], preferred_element_type=jnp.float32)
    up = jnp.dot(flat, up_weight[0], preferred_element_type=jnp.float32)
    hidden = (jax.nn.silu(gate) * up).astype(jnp.bfloat16)
    part = jnp.dot(hidden, down_weight[0], preferred_element_type=jnp.float32)
    part = part.astype(jnp.bfloat16).reshape(SLICES, experts * capacity, tp_count, cols)
    part = jnp.transpose(part, (0, 2, 1, 3)).reshape(-1, experts * capacity, cols)
    parts = lax.all_to_all(part, GROUP_AXES, split_axis=0, concat_axis=0, tiled=True)
    summed = jnp.sum(parts.astype(jnp.float32), axis=0).astype(jnp.bfloat16)
    summed = summed.reshape(experts, capacity, cols)
    returned = lax.all_to_all(summed, EXPERT_AXES, split_axis=0, concat_axis=0, tiled=True)
    returned = returned.reshape(experts * capacity, cols).astype(jnp.float32)
    routed = jnp.dot(
        weighted, returned, precision=lax.Precision.HIGHEST, preferred_element_type=jnp.float32
    )
    return (residual_cols.astype(jnp.float32) + routed).astype(jnp.bfloat16)


def solution(mesh):
    half = mesh.shape["ep"] // (2 * SLICES)
    fine = Mesh(
        mesh.devices.reshape(half, 2, 2, 2, mesh.shape["tp"]), EP_AXES + ("tp",)
    )
    return jax.shard_map(
        body,
        mesh=fine,
        in_specs=(
            P(EP_AXES, None),
            P(),
            P(None, "tp"),
            P(None, "tp"),
            P(None, "tp"),
            P(None, "tp"),
            P("tp"),
            P("tp", None),
            P(EP_AXES, "tp", None, None),
            P(EP_AXES, "tp", None, None),
            P(EP_AXES, "tp", None),
            P(EP_AXES),
            P(),
            P(EP_AXES, None),
            P(EP_AXES, None),
            P(EP_AXES, None, "tp"),
            P(EP_AXES, None, "tp"),
            P(EP_AXES, "tp", None),
        ),
        out_specs=P(EP_AXES, "tp"),
        check_vma=False,
    )
```

```python
import functools

import jax
import jax.numpy as jnp
from jax import lax
from jax.experimental import pallas as pl
from jax.experimental.pallas import tpu as pltpu
from jax.sharding import Mesh
from jax.sharding import PartitionSpec as P

HEADS = 8
KVH = 4
HD = 64
SLICES = 4
TOP_K = 2
STORED_SPAN = 1024


EPSILON = 1e-06
EXPERT_AXES = ("z", "xh")
SLICE_AXES = ("xl", "core")
EP_AXES = EXPERT_AXES + SLICE_AXES
GROUP_AXES = SLICE_AXES + ("tp",)


def copy_for_each(shard, axis):
    copies = jnp.broadcast_to(shard, (lax.axis_size(axis), *shard.shape))
    return lax.all_to_all(copies, axis, split_axis=0, concat_axis=0, tiled=True)


def attention_kernel(
    lengths,
    bias,
    tokens,
    gain,
    wq,
    wk,
    wv,
    wf,
    wo,
    cumul,
    keys,
    values,
    out,
    key_buf,
    value_buf,
    cum_rows,
    token_rows,
    key_sems,
    value_sems,
    *,
    seq_rows,
    pad,
    chunk,
):
    span = keys.shape[1]
    total_rows = seq_rows * HD
    width = tokens.shape[1]
    starts = list(range(0, total_rows, chunk))

    def copies(source, buf, sems):
        return [
            pltpu.make_async_copy(
                source.at[pl.ds(r, min(chunk, total_rows - r))],
                buf.at[pl.ds(r, min(chunk, total_rows - r))],
                sems.at[i],
            )
            for i, r in enumerate(starts)
        ]

    key_copies = copies(keys, key_buf, key_sems)
    value_copies = copies(values, value_buf, value_sems)
    for copy in key_copies + value_copies:
        copy.start()

    f32 = jnp.float32
    bf16 = jnp.bfloat16
    nt = (((1,), (1,)), ((), ()))
    token_rows[...] = jnp.zeros_like(token_rows)
    token_rows[0:seq_rows, :] = tokens[...].astype(f32)
    cum_rows[...] = jnp.zeros_like(cum_rows)
    for b in range(seq_rows):
        pair = cumul[b]
        cum_rows[b : b + 1, :] = pair[0:1, :]
        cum_rows[pad + b : pad + b + 1, :] = pair[1:2, :]

    rows = token_rows[...]
    inv = lax.rsqrt(jnp.sum(rows * rows, axis=-1, keepdims=True) / width + EPSILON)
    normed_f = (rows * inv * gain[...]).astype(bf16).astype(f32)
    normed = normed_f.astype(bf16)
    query = jnp.dot(normed, wq[...], preferred_element_type=f32).astype(bf16).astype(f32)
    fresh = lax.dot_general(normed, wk[...], nt, preferred_element_type=f32)
    fresh = fresh.astype(bf16).astype(f32)
    new_values = lax.dot_general(normed, wv[...], nt, preferred_element_type=f32)
    new_values = new_values.astype(bf16).astype(f32)
    wf_rows = wf[...].astype(f32)
    forget = []
    for g in range(2):
        raw = jnp.sum(normed_f * wf_rows[g : g + 1, :], axis=-1, keepdims=True) + bias[g]
        forget.append(jnp.minimum(raw, 0.0) - jnp.log1p(jnp.exp(-jnp.abs(raw))))
    log_forget = jnp.concatenate(forget, axis=0)

    scale = HD ** (-0.5)
    own = jnp.concatenate(
        [
            jnp.sum(query[:, g * HD : (g + 1) * HD] * fresh, axis=-1, keepdims=True)
            for g in range(2)
        ],
        axis=0,
    )
    own = own * scale

    swapped = pltpu.roll(query, HD, 1)
    low = lax.broadcasted_iota(jnp.int32, query.shape, 1) < HD
    both = jnp.concatenate([jnp.where(low, query, swapped), jnp.where(low, swapped, query)], axis=0)
    both = both * scale
    row_seq = lax.broadcasted_iota(jnp.int32, (2 * pad, 1), 0)
    row_seq = jnp.where(row_seq >= pad, row_seq - pad, row_seq)
    scores = jnp.zeros((2 * pad, span), f32)
    for i, r in enumerate(starts):
        size = min(chunk, total_rows - r)
        parts = [both] * (size // (2 * HD)) + ([both[:, :HD]] if size % (2 * HD) else [])
        left = jnp.concatenate(parts, axis=1) if len(parts) > 1 else parts[0]
        seq = lax.broadcasted_iota(jnp.int32, (1, size), 1) // HD + r // HD
        left = jnp.where(seq == row_seq, left, 0.0).astype(bf16)
        key_copies[i].wait()
        scores = scores + jnp.dot(left, key_buf[r : r + size, :], preferred_element_type=f32)

    limit = jnp.zeros((2 * pad, 1), jnp.int32)
    for b in range(seq_rows):
        limit = jnp.where(row_seq == b, lengths[b], limit)
    position = lax.broadcasted_iota(jnp.int32, (1, span), 1)
    cum = cum_rows[...]
    last = jnp.sum(jnp.where(position == limit - 1, cum, 0.0), axis=-1, keepdims=True)
    scores = jnp.where(position < limit, scores + (last - cum) + log_forget, -jnp.inf)
    top = jnp.maximum(jnp.max(scores, axis=-1, keepdims=True), own)
    expo = jnp.exp(scores - top)
    own_exp = jnp.exp(own - top)
    total = jnp.sum(expo, axis=-1, keepdims=True) + own_exp
    weights = (expo / total).astype(bf16)
    own_weight = (own_exp / total).astype(bf16).astype(f32)

    folded = jnp.zeros((2 * pad, 2 * HD), f32)
    for i, r in enumerate(starts):
        size = min(chunk, total_rows - r)
        value_copies[i].wait()
        wide = lax.dot_general(
            weights, value_buf[r : r + size, :], nt, preferred_element_type=f32
        )
        seq = lax.broadcasted_iota(jnp.int32, (1, size), 1) // HD + r // HD
        wide = jnp.where(seq == row_seq, wide, 0.0)
        for c in range(0, size, 2 * HD):
            piece = wide[:, c : min(c + 2 * HD, size)]
            if piece.shape[1] < 2 * HD:
                piece = jnp.concatenate([piece, jnp.zeros_like(piece)], axis=1)
            folded = folded + piece
    mixed = folded + pltpu.roll(folded, HD, 1)
    mixed = mixed + own_weight * jnp.concatenate(
        [jnp.concatenate([new_values, new_values], axis=1)] * 2, axis=0
    )
    heads = jnp.where(low, mixed[0:pad, :], mixed[pad : 2 * pad, :]).astype(bf16)
    partial = jnp.dot(heads, wo[...], preferred_element_type=f32).astype(bf16)
    blocks = out.shape[0]
    cols = out.shape[2]
    for n in range(blocks):
        out[n] = partial[0:seq_rows, n * cols : (n + 1) * cols]


def attention_call(
    tokens,
    gain,
    wq,
    wk,
    wv,
    wf,
    bias,
    wo,
    keys,
    values,
    cumul,
    lengths,
    blocks,
):
    seq_rows, width = tokens.shape
    span = keys.shape[3]
    pad = 16
    chunk = 4 * HD
    count = -(-seq_rows * HD // chunk)
    vmem = pl.BlockSpec(memory_space=pltpu.VMEM)
    smem = pl.BlockSpec(memory_space=pltpu.SMEM)
    hbm = pl.BlockSpec(memory_space=pl.ANY)
    kernel = functools.partial(attention_kernel, seq_rows=seq_rows, pad=pad, chunk=chunk)
    return pl.pallas_call(
        kernel,
        out_shape=jax.ShapeDtypeStruct((blocks, seq_rows, width // blocks), jnp.bfloat16),
        in_specs=[smem, smem] + [vmem] * 8 + [hbm, hbm],
        out_specs=vmem,
        scratch_shapes=[
            pltpu.VMEM((seq_rows * HD, span), jnp.bfloat16),
            pltpu.VMEM((seq_rows * HD, span), jnp.bfloat16),
            pltpu.VMEM((2 * pad, span), jnp.float32),
            pltpu.VMEM((pad, width), jnp.float32),
            pltpu.SemaphoreType.DMA((count,)),
            pltpu.SemaphoreType.DMA((count,)),
        ],
        name="attention",
    )(
        lengths,
        bias,
        tokens,
        gain.reshape(1, width),
        wq,
        wk.T,
        wv.T,
        wf.T,
        wo,
        cumul,
        keys.reshape(seq_rows * HD, span),
        values.reshape(seq_rows * HD, span),
    )


def expert_kernel(rows, gain, wg, wu, wd, out):
    f32 = jnp.float32
    bf16 = jnp.bfloat16
    peers, count, cols = rows.shape
    blocks = peers // SLICES
    width = blocks * cols
    pieces = []
    squares = 0.0
    for n in range(blocks):
        piece = jnp.concatenate([rows[s * blocks + n] for s in range(SLICES)], axis=0).astype(f32)
        squares = squares + jnp.sum(piece * piece, axis=-1, keepdims=True)
        pieces.append(piece)
    inv = lax.rsqrt(squares / width + EPSILON)
    gate = 0.0
    up = 0.0
    for n in range(blocks):
        span = slice(n * cols, (n + 1) * cols)
        flat = (pieces[n] * inv * gain[:, span]).astype(bf16)
        gate = gate + jnp.dot(flat, wg[span, :], preferred_element_type=f32)
        up = up + jnp.dot(flat, wu[span, :], preferred_element_type=f32)
    hidden = (gate / (1.0 + jnp.exp(-gate)) * up).astype(bf16)
    for n in range(blocks):
        span = slice(n * cols, (n + 1) * cols)
        part = jnp.dot(hidden, wd[:, span], preferred_element_type=f32).astype(bf16)
        for s in range(SLICES):
            out[s * blocks + n] = part[s * count : (s + 1) * count, :]


def expert_call(rows, gain, wg, wu, wd):
    vmem = pl.BlockSpec(memory_space=pltpu.VMEM)
    return pl.pallas_call(
        expert_kernel,
        out_shape=jax.ShapeDtypeStruct(rows.shape, jnp.bfloat16),
        in_specs=[vmem] * 5,
        out_specs=vmem,
        name="expert",
    )(rows, gain.reshape(1, -1), wg, wu, wd)


def slot_tables(routes, route_weights, experts, capacity):
    seq_rows = routes.shape[0]
    expert = lax.broadcasted_iota(jnp.int32, (experts, 1, 1), 0)
    chosen = routes[None] == expert
    named = jnp.any(chosen, axis=2).astype(jnp.float32)
    share = jnp.sum(jnp.where(chosen, route_weights[None], 0.0), axis=2)
    first = lax.broadcasted_iota(jnp.int32, (seq_rows, seq_rows), 0)
    second = lax.broadcasted_iota(jnp.int32, (seq_rows, seq_rows), 1)
    earlier = jnp.dot(named, (first < second).astype(jnp.float32))
    slot = lax.broadcasted_iota(jnp.int32, (1, capacity, 1), 1).astype(jnp.float32)
    here = (earlier[:, None, :] == slot) & (named[:, None, :] > 0.0)
    place = here.astype(jnp.bfloat16).reshape(experts * capacity, seq_rows)
    weighted = jnp.where(here, share[:, None, :], 0.0).reshape(experts * capacity, seq_rows)
    return place, weighted.T


def body(
    tokens,
    attn_gain,
    query_weight,
    key_weight,
    value_weight,
    forget_weight,
    forget_bias,
    out_weight,
    key_cache,
    value_cache,
    cum_forget,
    lengths,
    ffn_gain,
    routes,
    route_weights,
    gate_weight,
    up_weight,
    down_weight,
):
    tp_count = lax.axis_size("tp")
    ep_count = lax.axis_size(EXPERT_AXES) * SLICES
    tp_rank = lax.axis_index("tp")
    seq_rows = tokens.shape[0]
    width = tokens.shape[1]
    cols = width // tp_count
    experts = ep_count // SLICES
    capacity = min(seq_rows, max(2, (2 * seq_rows * TOP_K + experts - 1) // experts))
    partial = attention_call(
        tokens,
        attn_gain,
        query_weight,
        key_weight,
        value_weight,
        forget_weight,
        forget_bias,
        out_weight,
        key_cache,
        value_cache,
        cum_forget,
        lengths,
        tp_count,
    )
    blocks = lax.all_to_all(partial, "tp", 0, 0, tiled=True)
    mixed_cols = jnp.sum(blocks.astype(jnp.float32), axis=0)
    token_f = tokens.astype(jnp.float32)
    token_cols = lax.dynamic_slice_in_dim(token_f, tp_rank * cols, cols, 1)
    residual_cols = (token_cols + mixed_cols).astype(jnp.bfloat16)
    place, weighted = slot_tables(routes, route_weights, experts, capacity)
    outgoing = jnp.dot(place, residual_cols, preferred_element_type=jnp.float32)
    outgoing = outgoing.astype(jnp.bfloat16).reshape(experts, capacity, cols)
    arrived = lax.all_to_all(outgoing, EXPERT_AXES, split_axis=0, concat_axis=0, tiled=True)
    arrived = arrived.reshape(experts * capacity, cols)
    gathered = copy_for_each(arrived, GROUP_AXES)
    part = expert_call(gathered, ffn_gain, gate_weight[0], up_weight[0], down_weight[0])
    parts = lax.all_to_all(part, GROUP_AXES, split_axis=0, concat_axis=0, tiled=True)
    summed = jnp.sum(parts.astype(jnp.float32), axis=0).astype(jnp.bfloat16)
    summed = summed.reshape(experts, capacity, cols)
    returned = lax.all_to_all(summed, EXPERT_AXES, split_axis=0, concat_axis=0, tiled=True)
    returned = returned.reshape(experts * capacity, cols).astype(jnp.float32)
    routed = jnp.dot(
        weighted, returned, precision=lax.Precision.HIGHEST, preferred_element_type=jnp.float32
    )
    return (residual_cols.astype(jnp.float32) + routed).astype(jnp.bfloat16)


def solution(mesh):
    half = mesh.shape["ep"] // (2 * SLICES)
    fine = Mesh(
        mesh.devices.reshape(half, 2, 2, 2, mesh.shape["tp"]), EP_AXES + ("tp",)
    )
    return jax.shard_map(
        body,
        mesh=fine,
        in_specs=(
            P(EP_AXES, None),
            P(),
            P(None, "tp"),
            P(None, "tp"),
            P(None, "tp"),
            P(None, "tp"),
            P("tp"),
            P("tp", None),
            P(EP_AXES, "tp", None, None),
            P(EP_AXES, "tp", None, None),
            P(EP_AXES, "tp", None),
            P(EP_AXES),
            P(),
            P(EP_AXES, None),
            P(EP_AXES, None),
            P(EP_AXES, None, "tp"),
            P(EP_AXES, None, "tp"),
            P(EP_AXES, "tp", None),
        ),
        out_specs=P(EP_AXES, "tp"),
        check_vma=False,
    )
```

```python
import functools

import jax
import jax.numpy as jnp
from jax import lax
from jax.experimental import pallas as pl
from jax.experimental.pallas import tpu as pltpu
from jax.sharding import Mesh
from jax.sharding import PartitionSpec as P

HEADS = 8
KVH = 4
HD = 64
SLICES = 4
TOP_K = 2
STORED_SPAN = 1024


EPSILON = 1e-06
EXPERT_AXES = ("z", "xh")
SLICE_AXES = ("xl", "core")
EP_AXES = EXPERT_AXES + SLICE_AXES
GROUP_AXES = ("xl", "tp")


def copy_for_each(shard, axis):
    copies = jnp.broadcast_to(shard, (lax.axis_size(axis), *shard.shape))
    return lax.all_to_all(copies, axis, split_axis=0, concat_axis=0, tiled=True)


def attention_kernel(
    lengths,
    bias,
    tokens,
    gain,
    wq,
    wk,
    wv,
    wf,
    wo,
    cumul,
    keys,
    values,
    wg,
    wu,
    wd,
    out,
    pack,
    key_buf,
    value_buf,
    cum_rows,
    token_rows,
    key_sems,
    value_sems,
    pack_sems,
    *,
    seq_rows,
    pad,
    chunk,
):
    span = keys.shape[1]
    total_rows = seq_rows * HD
    width = tokens.shape[1]
    starts = list(range(0, total_rows, chunk))

    def copies(source, buf, sems):
        return [
            pltpu.make_async_copy(
                source.at[pl.ds(r, min(chunk, total_rows - r))],
                buf.at[pl.ds(r, min(chunk, total_rows - r))],
                sems.at[i],
            )
            for i, r in enumerate(starts)
        ]

    key_copies = copies(keys, key_buf, key_sems)
    value_copies = copies(values, value_buf, value_sems)
    units = wg.shape[1]
    pack_copies = [
        pltpu.make_async_copy(wg, pack.at[0], pack_sems.at[0]),
        pltpu.make_async_copy(wu, pack.at[1], pack_sems.at[1]),
    ] + [
        pltpu.make_async_copy(
            wd.at[:, pl.ds(j * units, units)],
            pack.at[2, pl.ds(j * units, units), :],
            pack_sems.at[2 + j],
        )
        for j in range(wd.shape[1] // units)
    ]
    for copy in key_copies + value_copies + pack_copies:
        copy.start()

    f32 = jnp.float32
    bf16 = jnp.bfloat16
    nt = (((1,), (1,)), ((), ()))
    token_rows[...] = jnp.zeros_like(token_rows)
    token_rows[0:seq_rows, :] = tokens[...].astype(f32)
    cum_rows[...] = jnp.zeros_like(cum_rows)
    for b in range(seq_rows):
        pair = cumul[b]
        cum_rows[b : b + 1, :] = pair[0:1, :]
        cum_rows[pad + b : pad + b + 1, :] = pair[1:2, :]

    rows = token_rows[...]
    inv = lax.rsqrt(jnp.sum(rows * rows, axis=-1, keepdims=True) / width + EPSILON)
    normed_f = (rows * inv * gain[...]).astype(bf16).astype(f32)
    normed = normed_f.astype(bf16)
    query = jnp.dot(normed, wq[...], preferred_element_type=f32).astype(bf16).astype(f32)
    fresh = lax.dot_general(normed, wk[...], nt, preferred_element_type=f32)
    fresh = fresh.astype(bf16).astype(f32)
    new_values = lax.dot_general(normed, wv[...], nt, preferred_element_type=f32)
    new_values = new_values.astype(bf16).astype(f32)
    wf_rows = wf[...].astype(f32)
    forget = []
    for g in range(2):
        raw = jnp.sum(normed_f * wf_rows[g : g + 1, :], axis=-1, keepdims=True) + bias[g]
        forget.append(jnp.minimum(raw, 0.0) - jnp.log1p(jnp.exp(-jnp.abs(raw))))
    log_forget = jnp.concatenate(forget, axis=0)

    scale = HD ** (-0.5)
    own = jnp.concatenate(
        [
            jnp.sum(query[:, g * HD : (g + 1) * HD] * fresh, axis=-1, keepdims=True)
            for g in range(2)
        ],
        axis=0,
    )
    own = own * scale

    swapped = pltpu.roll(query, HD, 1)
    low = lax.broadcasted_iota(jnp.int32, query.shape, 1) < HD
    both = jnp.concatenate([jnp.where(low, query, swapped), jnp.where(low, swapped, query)], axis=0)
    both = both * scale
    row_seq = lax.broadcasted_iota(jnp.int32, (2 * pad, 1), 0)
    row_seq = jnp.where(row_seq >= pad, row_seq - pad, row_seq)
    scores = jnp.zeros((2 * pad, span), f32)
    for i, r in enumerate(starts):
        size = min(chunk, total_rows - r)
        parts = [both] * (size // (2 * HD)) + ([both[:, :HD]] if size % (2 * HD) else [])
        left = jnp.concatenate(parts, axis=1) if len(parts) > 1 else parts[0]
        seq = lax.broadcasted_iota(jnp.int32, (1, size), 1) // HD + r // HD
        left = jnp.where(seq == row_seq, left, 0.0).astype(bf16)
        key_copies[i].wait()
        scores = scores + jnp.dot(left, key_buf[r : r + size, :], preferred_element_type=f32)

    limit = jnp.zeros((2 * pad, 1), jnp.int32)
    for b in range(seq_rows):
        limit = jnp.where(row_seq == b, lengths[b], limit)
    position = lax.broadcasted_iota(jnp.int32, (1, span), 1)
    cum = cum_rows[...]
    last = jnp.sum(jnp.where(position == limit - 1, cum, 0.0), axis=-1, keepdims=True)
    scores = jnp.where(position < limit, scores + (last - cum) + log_forget, -jnp.inf)
    top = jnp.maximum(jnp.max(scores, axis=-1, keepdims=True), own)
    expo = jnp.exp(scores - top)
    own_exp = jnp.exp(own - top)
    total = jnp.sum(expo, axis=-1, keepdims=True) + own_exp
    weights = (expo / total).astype(bf16)
    own_weight = (own_exp / total).astype(bf16).astype(f32)

    folded = jnp.zeros((2 * pad, 2 * HD), f32)
    for i, r in enumerate(starts):
        size = min(chunk, total_rows - r)
        value_copies[i].wait()
        wide = lax.dot_general(
            weights, value_buf[r : r + size, :], nt, preferred_element_type=f32
        )
        seq = lax.broadcasted_iota(jnp.int32, (1, size), 1) // HD + r // HD
        wide = jnp.where(seq == row_seq, wide, 0.0)
        for c in range(0, size, 2 * HD):
            piece = wide[:, c : min(c + 2 * HD, size)]
            if piece.shape[1] < 2 * HD:
                piece = jnp.concatenate([piece, jnp.zeros_like(piece)], axis=1)
            folded = folded + piece
    mixed = folded + pltpu.roll(folded, HD, 1)
    mixed = mixed + own_weight * jnp.concatenate(
        [jnp.concatenate([new_values, new_values], axis=1)] * 2, axis=0
    )
    heads = jnp.where(low, mixed[0:pad, :], mixed[pad : 2 * pad, :]).astype(bf16)
    partial = jnp.dot(heads, wo[...], preferred_element_type=f32).astype(bf16)
    blocks = out.shape[0]
    cols = out.shape[2]
    for n in range(blocks):
        out[n] = partial[0:seq_rows, n * cols : (n + 1) * cols]
    for copy in pack_copies:
        copy.wait()


def attention_call(
    tokens,
    gain,
    wq,
    wk,
    wv,
    wf,
    bias,
    wo,
    keys,
    values,
    cumul,
    lengths,
    wg,
    wu,
    wd,
    blocks,
):
    seq_rows, width = tokens.shape
    span = keys.shape[3]
    pad = 16
    chunk = 4 * HD
    count = -(-seq_rows * HD // chunk)
    vmem = pl.BlockSpec(memory_space=pltpu.VMEM)
    smem = pl.BlockSpec(memory_space=pltpu.SMEM)
    hbm = pl.BlockSpec(memory_space=pl.ANY)
    kernel = functools.partial(attention_kernel, seq_rows=seq_rows, pad=pad, chunk=chunk)
    return pl.pallas_call(
        kernel,
        out_shape=(
            jax.ShapeDtypeStruct((blocks, seq_rows, width // blocks), jnp.bfloat16),
            jax.ShapeDtypeStruct((3,) + wg.shape, jnp.bfloat16),
        ),
        in_specs=[smem, smem] + [vmem] * 8 + [hbm] * 5,
        out_specs=(vmem, hbm),
        scratch_shapes=[
            pltpu.VMEM((seq_rows * HD, span), jnp.bfloat16),
            pltpu.VMEM((seq_rows * HD, span), jnp.bfloat16),
            pltpu.VMEM((2 * pad, span), jnp.float32),
            pltpu.VMEM((pad, width), jnp.float32),
            pltpu.SemaphoreType.DMA((count,)),
            pltpu.SemaphoreType.DMA((count,)),
            pltpu.SemaphoreType.DMA((2 + width // wg.shape[1],)),
        ],
        name="attention",
    )(
        lengths,
        bias,
        tokens,
        gain.reshape(1, width),
        wq,
        wk.T,
        wv.T,
        wf.T,
        wo,
        cumul,
        keys.reshape(seq_rows * HD, span),
        values.reshape(seq_rows * HD, span),
        wg,
        wu,
        wd,
    )


def expert_kernel(
    rows, gain, own, other, out, row_buf, own_buf, other_buf, row_sem, own_sems, other_sems
):
    f32 = jnp.float32
    bf16 = jnp.bfloat16
    peers, count, cols = rows.shape
    width = gain.shape[1]
    blocks = width // cols
    groups = peers // blocks
    units = own.shape[2]
    row_copy = pltpu.make_async_copy(rows, row_buf, row_sem)
    row_copy.start()
    own_copies = [pltpu.make_async_copy(own.at[i], own_buf.at[i], own_sems.at[i]) for i in range(3)]
    other_copies = [
        pltpu.make_async_copy(other.at[i], other_buf.at[i], other_sems.at[i]) for i in range(3)
    ]
    for i in range(3):
        own_copies[i].start()
        other_copies[i].start()
    row_copy.wait()
    pieces = []
    squares = 0.0
    for n in range(blocks):
        piece = jnp.concatenate([row_buf[s * blocks + n] for s in range(groups)], axis=0)
        piece = piece.astype(f32)
        squares = squares + jnp.sum(piece * piece, axis=-1, keepdims=True)
        pieces.append(piece)
    inv = lax.rsqrt(squares / width + EPSILON)
    flats = [
        (pieces[n] * inv * gain[:, n * cols : (n + 1) * cols]).astype(bf16) for n in range(blocks)
    ]

    def projected(i):
        own_copies[i].wait()
        other_copies[i].wait()
        total = 0.0
        for n in range(blocks):
            span = slice(n * cols, (n + 1) * cols)
            weight = jnp.concatenate([own_buf[i, span, :], other_buf[i, span, :]], axis=1)
            total = total + jnp.dot(flats[n], weight, preferred_element_type=f32)
        return total

    gate = projected(0)
    up = projected(1)
    hidden = (gate / (1.0 + jnp.exp(-gate)) * up).astype(bf16)
    own_copies[2].wait()
    other_copies[2].wait()
    for n in range(blocks):
        strips = []
        for j in range(n * cols // units, (n + 1) * cols // units):
            span = slice(j * units, (j + 1) * units)
            strips.append(jnp.concatenate([own_buf[2, span, :], other_buf[2, span, :]], axis=0))
        weight = jnp.concatenate(strips, axis=1)
        part = jnp.dot(hidden, weight, preferred_element_type=f32).astype(bf16)
        for s in range(groups):
            out[s * blocks + n] = part[s * count : (s + 1) * count, :]


def expert_call(rows, gain, own, other):
    vmem = pl.BlockSpec(memory_space=pltpu.VMEM)
    hbm = pl.BlockSpec(memory_space=pl.ANY)
    return pl.pallas_call(
        expert_kernel,
        out_shape=jax.ShapeDtypeStruct(rows.shape, jnp.bfloat16),
        in_specs=[hbm, vmem, hbm, hbm],
        out_specs=vmem,
        scratch_shapes=[
            pltpu.VMEM(rows.shape, jnp.bfloat16),
            pltpu.VMEM(own.shape, jnp.bfloat16),
            pltpu.VMEM(own.shape, jnp.bfloat16),
            pltpu.SemaphoreType.DMA,
            pltpu.SemaphoreType.DMA((3,)),
            pltpu.SemaphoreType.DMA((3,)),
        ],
        name="expert",
    )(rows, gain.reshape(1, -1), own, other)


def slot_tables(routes, route_weights, experts, capacity):
    seq_rows = routes.shape[0]
    expert = lax.broadcasted_iota(jnp.int32, (experts, 1, 1), 0)
    chosen = routes[None] == expert
    named = jnp.any(chosen, axis=2).astype(jnp.float32)
    share = jnp.sum(jnp.where(chosen, route_weights[None], 0.0), axis=2)
    first = lax.broadcasted_iota(jnp.int32, (seq_rows, seq_rows), 0)
    second = lax.broadcasted_iota(jnp.int32, (seq_rows, seq_rows), 1)
    earlier = jnp.dot(named, (first < second).astype(jnp.float32))
    slot = lax.broadcasted_iota(jnp.int32, (1, capacity, 1), 1).astype(jnp.float32)
    here = (earlier[:, None, :] == slot) & (named[:, None, :] > 0.0)
    place = here.astype(jnp.bfloat16).reshape(experts * capacity, seq_rows)
    weighted = jnp.where(here, share[:, None, :], 0.0).reshape(experts * capacity, seq_rows)
    return place, weighted.T


def body(
    tokens,
    attn_gain,
    query_weight,
    key_weight,
    value_weight,
    forget_weight,
    forget_bias,
    out_weight,
    key_cache,
    value_cache,
    cum_forget,
    lengths,
    ffn_gain,
    routes,
    route_weights,
    gate_weight,
    up_weight,
    down_weight,
):
    tp_count = lax.axis_size("tp")
    ep_count = lax.axis_size(EXPERT_AXES) * SLICES
    tp_rank = lax.axis_index("tp")
    seq_rows = tokens.shape[0]
    width = tokens.shape[1]
    cols = width // tp_count
    experts = ep_count // SLICES
    capacity = min(seq_rows, max(2, (2 * seq_rows * TOP_K + experts - 1) // experts))
    partial, own_pack = attention_call(
        tokens,
        attn_gain,
        query_weight,
        key_weight,
        value_weight,
        forget_weight,
        forget_bias,
        out_weight,
        key_cache,
        value_cache,
        cum_forget,
        lengths,
        gate_weight[0],
        up_weight[0],
        down_weight[0],
        tp_count,
    )
    other_pack = lax.ppermute(own_pack, "core", [(0, 1), (1, 0)])
    blocks = lax.all_to_all(partial, "tp", 0, 0, tiled=True)
    mixed_cols = jnp.sum(blocks.astype(jnp.float32), axis=0)
    token_f = tokens.astype(jnp.float32)
    token_cols = lax.dynamic_slice_in_dim(token_f, tp_rank * cols, cols, 1)
    residual_cols = (token_cols + mixed_cols).astype(jnp.bfloat16)
    place, weighted = slot_tables(routes, route_weights, experts, capacity)
    outgoing = jnp.dot(place, residual_cols, preferred_element_type=jnp.float32)
    outgoing = outgoing.astype(jnp.bfloat16).reshape(experts, capacity, cols)
    arrived = lax.all_to_all(outgoing, EXPERT_AXES, split_axis=0, concat_axis=0, tiled=True)
    arrived = arrived.reshape(experts * capacity, cols)
    arrived, other_pack = lax.optimization_barrier((arrived, other_pack))
    gathered = copy_for_each(arrived, GROUP_AXES)
    part = expert_call(gathered, ffn_gain, own_pack, other_pack)
    parts = lax.all_to_all(part, GROUP_AXES, split_axis=0, concat_axis=0, tiled=True)
    summed = jnp.sum(parts.astype(jnp.float32), axis=0).astype(jnp.bfloat16)
    summed = summed.reshape(experts, capacity, cols)
    returned = lax.all_to_all(summed, EXPERT_AXES, split_axis=0, concat_axis=0, tiled=True)
    returned = returned.reshape(experts * capacity, cols).astype(jnp.float32)
    routed = jnp.dot(
        weighted, returned, precision=lax.Precision.HIGHEST, preferred_element_type=jnp.float32
    )
    return (residual_cols.astype(jnp.float32) + routed).astype(jnp.bfloat16)


def solution(mesh):
    half = mesh.shape["ep"] // (2 * SLICES)
    fine = Mesh(
        mesh.devices.reshape(half, 2, 2, 2, mesh.shape["tp"]), EP_AXES + ("tp",)
    )
    return jax.shard_map(
        body,
        mesh=fine,
        in_specs=(
            P(EP_AXES, None),
            P(),
            P(None, "tp"),
            P(None, "tp"),
            P(None, "tp"),
            P(None, "tp"),
            P("tp"),
            P("tp", None),
            P(EP_AXES, "tp", None, None),
            P(EP_AXES, "tp", None, None),
            P(EP_AXES, "tp", None),
            P(EP_AXES),
            P(),
            P(EP_AXES, None),
            P(EP_AXES, None),
            P(EP_AXES, None, "tp"),
            P(EP_AXES, None, "tp"),
            P(EP_AXES, "tp", None),
        ),
        out_specs=P(EP_AXES, "tp"),
        check_vma=False,
    )
```

```python
import functools

import jax
import jax.numpy as jnp
from jax import lax
from jax.experimental import pallas as pl
from jax.experimental.pallas import tpu as pltpu
from jax.sharding import Mesh
from jax.sharding import PartitionSpec as P

HEADS = 8
KVH = 4
HD = 64
SLICES = 4
TOP_K = 2
STORED_SPAN = 1024


EPSILON = 1e-06
EXPERT_AXES = ("z", "xh")
SLICE_AXES = ("xl", "core")
EP_AXES = EXPERT_AXES + SLICE_AXES
GROUP_AXES = ("xl", "tp")


def copy_for_each(shard, axis):
    copies = jnp.broadcast_to(shard, (lax.axis_size(axis), *shard.shape))
    return lax.all_to_all(copies, axis, split_axis=0, concat_axis=0, tiled=True)


def attention_kernel(
    lengths,
    bias,
    tokens,
    gain,
    wq,
    wk,
    wv,
    wf,
    wo,
    cumul,
    keys,
    values,
    wg,
    wu,
    wd,
    out,
    pack,
    key_buf,
    value_buf,
    pack_buf,
    cum_rows,
    token_rows,
    key_sems,
    value_sems,
    pack_sems,
    *,
    seq_rows,
    pad,
    chunk,
):
    span = keys.shape[1]
    total_rows = seq_rows * HD
    width = tokens.shape[1]
    starts = list(range(0, total_rows, chunk))

    def copies(source, buf, sems):
        return [
            pltpu.make_async_copy(
                source.at[pl.ds(r, min(chunk, total_rows - r))],
                buf.at[pl.ds(r, min(chunk, total_rows - r))],
                sems.at[i],
            )
            for i, r in enumerate(starts)
        ]

    key_copies = copies(keys, key_buf, key_sems)
    value_copies = copies(values, value_buf, value_sems)
    units = wg.shape[1]
    pack_loads = [
        pltpu.make_async_copy(wg, pack_buf.at[0], pack_sems.at[0]),
        pltpu.make_async_copy(wu, pack_buf.at[1], pack_sems.at[1]),
    ] + [
        pltpu.make_async_copy(
            wd.at[:, pl.ds(j * units, units)],
            pack_buf.at[2, pl.ds(j * units, units), :],
            pack_sems.at[2 + j],
        )
        for j in range(wd.shape[1] // units)
    ]
    pack_store = pltpu.make_async_copy(pack_buf, pack, pack_sems.at[len(pack_loads)])
    for copy in key_copies + value_copies + pack_loads:
        copy.start()

    f32 = jnp.float32
    bf16 = jnp.bfloat16
    nt = (((1,), (1,)), ((), ()))
    token_rows[...] = jnp.zeros_like(token_rows)
    token_rows[0:seq_rows, :] = tokens[...].astype(f32)
    cum_rows[...] = jnp.zeros_like(cum_rows)
    for b in range(seq_rows):
        pair = cumul[b]
        cum_rows[b : b + 1, :] = pair[0:1, :]
        cum_rows[pad + b : pad + b + 1, :] = pair[1:2, :]

    rows = token_rows[...]
    inv = lax.rsqrt(jnp.sum(rows * rows, axis=-1, keepdims=True) / width + EPSILON)
    normed_f = (rows * inv * gain[...]).astype(bf16).astype(f32)
    normed = normed_f.astype(bf16)
    query = jnp.dot(normed, wq[...], preferred_element_type=f32).astype(bf16).astype(f32)
    fresh = lax.dot_general(normed, wk[...], nt, preferred_element_type=f32)
    fresh = fresh.astype(bf16).astype(f32)
    new_values = lax.dot_general(normed, wv[...], nt, preferred_element_type=f32)
    new_values = new_values.astype(bf16).astype(f32)
    wf_rows = wf[...].astype(f32)
    forget = []
    for g in range(2):
        raw = jnp.sum(normed_f * wf_rows[g : g + 1, :], axis=-1, keepdims=True) + bias[g]
        forget.append(jnp.minimum(raw, 0.0) - jnp.log1p(jnp.exp(-jnp.abs(raw))))
    log_forget = jnp.concatenate(forget, axis=0)

    scale = HD ** (-0.5)
    own = jnp.concatenate(
        [
            jnp.sum(query[:, g * HD : (g + 1) * HD] * fresh, axis=-1, keepdims=True)
            for g in range(2)
        ],
        axis=0,
    )
    own = own * scale

    swapped = pltpu.roll(query, HD, 1)
    low = lax.broadcasted_iota(jnp.int32, query.shape, 1) < HD
    both = jnp.concatenate([jnp.where(low, query, swapped), jnp.where(low, swapped, query)], axis=0)
    both = both * scale
    row_seq = lax.broadcasted_iota(jnp.int32, (2 * pad, 1), 0)
    row_seq = jnp.where(row_seq >= pad, row_seq - pad, row_seq)
    scores = jnp.zeros((2 * pad, span), f32)
    for i, r in enumerate(starts):
        size = min(chunk, total_rows - r)
        parts = [both] * (size // (2 * HD)) + ([both[:, :HD]] if size % (2 * HD) else [])
        left = jnp.concatenate(parts, axis=1) if len(parts) > 1 else parts[0]
        seq = lax.broadcasted_iota(jnp.int32, (1, size), 1) // HD + r // HD
        left = jnp.where(seq == row_seq, left, 0.0).astype(bf16)
        key_copies[i].wait()
        scores = scores + jnp.dot(left, key_buf[r : r + size, :], preferred_element_type=f32)

    for copy in pack_loads:
        copy.wait()
    pack_store.start()

    limit = jnp.zeros((2 * pad, 1), jnp.int32)
    for b in range(seq_rows):
        limit = jnp.where(row_seq == b, lengths[b], limit)
    position = lax.broadcasted_iota(jnp.int32, (1, span), 1)
    cum = cum_rows[...]
    last = jnp.sum(jnp.where(position == limit - 1, cum, 0.0), axis=-1, keepdims=True)
    scores = jnp.where(position < limit, scores + (last - cum) + log_forget, -jnp.inf)
    top = jnp.maximum(jnp.max(scores, axis=-1, keepdims=True), own)
    expo = jnp.exp(scores - top)
    own_exp = jnp.exp(own - top)
    total = jnp.sum(expo, axis=-1, keepdims=True) + own_exp
    weights = (expo / total).astype(bf16)
    own_weight = (own_exp / total).astype(bf16).astype(f32)

    folded = jnp.zeros((2 * pad, 2 * HD), f32)
    for i, r in enumerate(starts):
        size = min(chunk, total_rows - r)
        value_copies[i].wait()
        wide = lax.dot_general(
            weights, value_buf[r : r + size, :], nt, preferred_element_type=f32
        )
        seq = lax.broadcasted_iota(jnp.int32, (1, size), 1) // HD + r // HD
        wide = jnp.where(seq == row_seq, wide, 0.0)
        for c in range(0, size, 2 * HD):
            piece = wide[:, c : min(c + 2 * HD, size)]
            if piece.shape[1] < 2 * HD:
                piece = jnp.concatenate([piece, jnp.zeros_like(piece)], axis=1)
            folded = folded + piece
    mixed = folded + pltpu.roll(folded, HD, 1)
    mixed = mixed + own_weight * jnp.concatenate(
        [jnp.concatenate([new_values, new_values], axis=1)] * 2, axis=0
    )
    heads = jnp.where(low, mixed[0:pad, :], mixed[pad : 2 * pad, :]).astype(bf16)
    partial = jnp.dot(heads, wo[...], preferred_element_type=f32).astype(bf16)
    blocks = out.shape[0]
    cols = out.shape[2]
    for n in range(blocks):
        out[n] = partial[0:seq_rows, n * cols : (n + 1) * cols]
    pack_store.wait()


def attention_call(
    tokens,
    gain,
    wq,
    wk,
    wv,
    wf,
    bias,
    wo,
    keys,
    values,
    cumul,
    lengths,
    wg,
    wu,
    wd,
    blocks,
):
    seq_rows, width = tokens.shape
    span = keys.shape[3]
    pad = 16
    chunk = 4 * HD
    count = -(-seq_rows * HD // chunk)
    vmem = pl.BlockSpec(memory_space=pltpu.VMEM)
    smem = pl.BlockSpec(memory_space=pltpu.SMEM)
    hbm = pl.BlockSpec(memory_space=pl.ANY)
    kernel = functools.partial(attention_kernel, seq_rows=seq_rows, pad=pad, chunk=chunk)
    return pl.pallas_call(
        kernel,
        out_shape=(
            jax.ShapeDtypeStruct((blocks, seq_rows, width // blocks), jnp.bfloat16),
            jax.ShapeDtypeStruct((3,) + wg.shape, jnp.bfloat16),
        ),
        in_specs=[smem, smem] + [vmem] * 8 + [hbm] * 5,
        out_specs=(vmem, hbm),
        scratch_shapes=[
            pltpu.VMEM((seq_rows * HD, span), jnp.bfloat16),
            pltpu.VMEM((seq_rows * HD, span), jnp.bfloat16),
            pltpu.VMEM((3,) + wg.shape, jnp.bfloat16),
            pltpu.VMEM((2 * pad, span), jnp.float32),
            pltpu.VMEM((pad, width), jnp.float32),
            pltpu.SemaphoreType.DMA((count,)),
            pltpu.SemaphoreType.DMA((count,)),
            pltpu.SemaphoreType.DMA((3 + width // wg.shape[1],)),
        ],
        name="attention",
    )(
        lengths,
        bias,
        tokens,
        gain.reshape(1, width),
        wq,
        wk.T,
        wv.T,
        wf.T,
        wo,
        cumul,
        keys.reshape(seq_rows * HD, span),
        values.reshape(seq_rows * HD, span),
        wg,
        wu,
        wd,
    )


def expert_kernel(
    rows, gain, own, other, out, row_buf, own_buf, other_buf, row_sem, own_sems, other_sems
):
    f32 = jnp.float32
    bf16 = jnp.bfloat16
    peers, count, cols = rows.shape
    width = gain.shape[1]
    blocks = width // cols
    groups = peers // blocks
    units = own.shape[2]
    row_copy = pltpu.make_async_copy(rows, row_buf, row_sem)
    row_copy.start()
    own_copies = [pltpu.make_async_copy(own.at[i], own_buf.at[i], own_sems.at[i]) for i in range(3)]
    other_copies = [
        pltpu.make_async_copy(other.at[i], other_buf.at[i], other_sems.at[i]) for i in range(3)
    ]
    for i in range(3):
        own_copies[i].start()
        other_copies[i].start()
    row_copy.wait()
    pieces = []
    squares = 0.0
    for n in range(blocks):
        piece = jnp.concatenate([row_buf[s * blocks + n] for s in range(groups)], axis=0)
        piece = piece.astype(f32)
        squares = squares + jnp.sum(piece * piece, axis=-1, keepdims=True)
        pieces.append(piece)
    inv = lax.rsqrt(squares / width + EPSILON)
    flats = [
        (pieces[n] * inv * gain[:, n * cols : (n + 1) * cols]).astype(bf16) for n in range(blocks)
    ]

    def projected(i):
        own_copies[i].wait()
        other_copies[i].wait()
        total = 0.0
        for n in range(blocks):
            span = slice(n * cols, (n + 1) * cols)
            weight = jnp.concatenate([own_buf[i, span, :], other_buf[i, span, :]], axis=1)
            total = total + jnp.dot(flats[n], weight, preferred_element_type=f32)
        return total

    gate = projected(0)
    up = projected(1)
    hidden = (gate / (1.0 + jnp.exp(-gate)) * up).astype(bf16)
    own_copies[2].wait()
    other_copies[2].wait()
    for n in range(blocks):
        strips = []
        for j in range(n * cols // units, (n + 1) * cols // units):
            span = slice(j * units, (j + 1) * units)
            strips.append(jnp.concatenate([own_buf[2, span, :], other_buf[2, span, :]], axis=0))
        weight = jnp.concatenate(strips, axis=1)
        part = jnp.dot(hidden, weight, preferred_element_type=f32).astype(bf16)
        for s in range(groups):
            out[s * blocks + n] = part[s * count : (s + 1) * count, :]


def expert_call(rows, gain, own, other):
    vmem = pl.BlockSpec(memory_space=pltpu.VMEM)
    hbm = pl.BlockSpec(memory_space=pl.ANY)
    return pl.pallas_call(
        expert_kernel,
        out_shape=jax.ShapeDtypeStruct(rows.shape, jnp.bfloat16),
        in_specs=[hbm, vmem, hbm, hbm],
        out_specs=vmem,
        scratch_shapes=[
            pltpu.VMEM(rows.shape, jnp.bfloat16),
            pltpu.VMEM(own.shape, jnp.bfloat16),
            pltpu.VMEM(own.shape, jnp.bfloat16),
            pltpu.SemaphoreType.DMA,
            pltpu.SemaphoreType.DMA((3,)),
            pltpu.SemaphoreType.DMA((3,)),
        ],
        name="expert",
    )(rows, gain.reshape(1, -1), own, other)


def slot_tables(routes, route_weights, experts, capacity):
    seq_rows = routes.shape[0]
    expert = lax.broadcasted_iota(jnp.int32, (experts, 1, 1), 0)
    chosen = routes[None] == expert
    named = jnp.any(chosen, axis=2).astype(jnp.float32)
    share = jnp.sum(jnp.where(chosen, route_weights[None], 0.0), axis=2)
    first = lax.broadcasted_iota(jnp.int32, (seq_rows, seq_rows), 0)
    second = lax.broadcasted_iota(jnp.int32, (seq_rows, seq_rows), 1)
    earlier = jnp.dot(named, (first < second).astype(jnp.float32))
    slot = lax.broadcasted_iota(jnp.int32, (1, capacity, 1), 1).astype(jnp.float32)
    here = (earlier[:, None, :] == slot) & (named[:, None, :] > 0.0)
    place = here.astype(jnp.bfloat16).reshape(experts * capacity, seq_rows)
    weighted = jnp.where(here, share[:, None, :], 0.0).reshape(experts * capacity, seq_rows)
    return place, weighted.T


def body(
    tokens,
    attn_gain,
    query_weight,
    key_weight,
    value_weight,
    forget_weight,
    forget_bias,
    out_weight,
    key_cache,
    value_cache,
    cum_forget,
    lengths,
    ffn_gain,
    routes,
    route_weights,
    gate_weight,
    up_weight,
    down_weight,
):
    tp_count = lax.axis_size("tp")
    ep_count = lax.axis_size(EXPERT_AXES) * SLICES
    tp_rank = lax.axis_index("tp")
    seq_rows = tokens.shape[0]
    width = tokens.shape[1]
    cols = width // tp_count
    experts = ep_count // SLICES
    capacity = min(seq_rows, max(2, (2 * seq_rows * TOP_K + experts - 1) // experts))
    partial, own_pack = attention_call(
        tokens,
        attn_gain,
        query_weight,
        key_weight,
        value_weight,
        forget_weight,
        forget_bias,
        out_weight,
        key_cache,
        value_cache,
        cum_forget,
        lengths,
        gate_weight[0],
        up_weight[0],
        down_weight[0],
        tp_count,
    )
    other_pack = lax.ppermute(own_pack, "core", [(0, 1), (1, 0)])
    blocks = lax.all_to_all(partial, "tp", 0, 0, tiled=True)
    mixed_cols = jnp.sum(blocks.astype(jnp.float32), axis=0)
    token_cols = lax.dynamic_slice_in_dim(tokens, tp_rank * cols, cols, 1)
    token_cols = lax.optimization_barrier(token_cols).astype(jnp.float32)
    residual_cols = (token_cols + mixed_cols).astype(jnp.bfloat16)
    place, weighted = slot_tables(routes, route_weights, experts, capacity)
    outgoing = jnp.dot(place, residual_cols, preferred_element_type=jnp.float32)
    outgoing = outgoing.astype(jnp.bfloat16).reshape(experts, capacity, cols)
    arrived = lax.all_to_all(outgoing, EXPERT_AXES, split_axis=0, concat_axis=0, tiled=True)
    arrived = arrived.reshape(experts * capacity, cols)
    arrived, other_pack = lax.optimization_barrier((arrived, other_pack))
    gathered = copy_for_each(arrived, GROUP_AXES)
    part = expert_call(gathered, ffn_gain, own_pack, other_pack)
    parts = lax.all_to_all(part, GROUP_AXES, split_axis=0, concat_axis=0, tiled=True)
    summed = jnp.sum(parts.astype(jnp.float32), axis=0).astype(jnp.bfloat16)
    summed = summed.reshape(experts, capacity, cols)
    returned = lax.all_to_all(summed, EXPERT_AXES, split_axis=0, concat_axis=0, tiled=True)
    returned = returned.reshape(experts * capacity, cols).astype(jnp.float32)
    routed = jnp.dot(
        weighted, returned, precision=lax.Precision.HIGHEST, preferred_element_type=jnp.float32
    )
    return (residual_cols.astype(jnp.float32) + routed).astype(jnp.bfloat16)


def solution(mesh):
    half = mesh.shape["ep"] // (2 * SLICES)
    fine = Mesh(
        mesh.devices.reshape(half, 2, 2, 2, mesh.shape["tp"]), EP_AXES + ("tp",)
    )
    return jax.shard_map(
        body,
        mesh=fine,
        in_specs=(
            P(EP_AXES, None),
            P(),
            P(None, "tp"),
            P(None, "tp"),
            P(None, "tp"),
            P(None, "tp"),
            P("tp"),
            P("tp", None),
            P(EP_AXES, "tp", None, None),
            P(EP_AXES, "tp", None, None),
            P(EP_AXES, "tp", None),
            P(EP_AXES),
            P(),
            P(EP_AXES, None),
            P(EP_AXES, None),
            P(EP_AXES, None, "tp"),
            P(EP_AXES, None, "tp"),
            P(EP_AXES, "tp", None),
        ),
        out_specs=P(EP_AXES, "tp"),
        check_vma=False,
    )
```

```python
import functools

import jax
import jax.numpy as jnp
from jax import lax
from jax.experimental import pallas as pl
from jax.experimental.pallas import tpu as pltpu
from jax.sharding import Mesh
from jax.sharding import PartitionSpec as P


HD = 64
SLICES = 4
TOP_K = 2


EPSILON = 1e-06
EXPERT_AXES = ("z", "xh")
SLICE_AXES = ("xl", "core")
EP_AXES = EXPERT_AXES + SLICE_AXES


def whole_exchange(blocks):
    return lax.all_to_all(blocks, ("tp",) + EXPERT_AXES, split_axis=0, concat_axis=0, tiled=True)


def attention_kernel(
    lengths,
    bias,
    tokens,
    gain,
    wq,
    wk,
    wv,
    wf,
    wo,
    cumul,
    keys,
    values,
    wg,
    wu,
    wd,
    out,
    pack,
    key_buf,
    value_buf,
    cum_rows,
    token_rows,
    key_sems,
    value_sems,
    pack_sems,
    *,
    seq_rows,
    pad,
    chunk,
):
    span = keys.shape[1]
    total_rows = seq_rows * HD
    width = tokens.shape[1]
    starts = list(range(0, total_rows, chunk))

    def copies(source, buf, sems):
        return [
            pltpu.make_async_copy(
                source.at[pl.ds(r, min(chunk, total_rows - r))],
                buf.at[pl.ds(r, min(chunk, total_rows - r))],
                sems.at[i],
            )
            for i, r in enumerate(starts)
        ]

    key_copies = copies(keys, key_buf, key_sems)
    value_copies = copies(values, value_buf, value_sems)
    units = wg.shape[1]
    pack_loads = [
        pltpu.make_async_copy(wg, pack.at[0], pack_sems.at[0]),
        pltpu.make_async_copy(wu, pack.at[1], pack_sems.at[1]),
    ] + [
        pltpu.make_async_copy(
            wd.at[:, pl.ds(j * units, units)],
            pack.at[2, pl.ds(j * units, units), :],
            pack_sems.at[2 + j],
        )
        for j in range(wd.shape[1] // units)
    ]
    for copy in key_copies + value_copies + pack_loads:
        copy.start()

    f32 = jnp.float32
    bf16 = jnp.bfloat16
    nt = (((1,), (1,)), ((), ()))
    token_rows[...] = jnp.zeros_like(token_rows)
    token_rows[0:seq_rows, :] = tokens[...].astype(f32)
    cum_rows[...] = jnp.zeros_like(cum_rows)
    for b in range(seq_rows):
        pair = cumul[b]
        cum_rows[b : b + 1, :] = pair[0:1, :]
        cum_rows[pad + b : pad + b + 1, :] = pair[1:2, :]

    rows = token_rows[...]
    inv = lax.rsqrt(jnp.sum(rows * rows, axis=-1, keepdims=True) / width + EPSILON)
    normed_f = (rows * inv * gain[...]).astype(bf16).astype(f32)
    normed = normed_f.astype(bf16)
    query = jnp.dot(normed, wq[...], preferred_element_type=f32).astype(bf16).astype(f32)
    fresh = lax.dot_general(normed, wk[...], nt, preferred_element_type=f32)
    fresh = fresh.astype(bf16).astype(f32)
    new_values = lax.dot_general(normed, wv[...], nt, preferred_element_type=f32)
    new_values = new_values.astype(bf16).astype(f32)
    wf_rows = wf[...].astype(f32)
    forget = []
    for g in range(2):
        raw = jnp.sum(normed_f * wf_rows[g : g + 1, :], axis=-1, keepdims=True) + bias[g]
        forget.append(jnp.minimum(raw, 0.0) - jnp.log1p(jnp.exp(-jnp.abs(raw))))
    log_forget = jnp.concatenate(forget, axis=0)

    scale = HD ** (-0.5)
    own = jnp.concatenate(
        [
            jnp.sum(query[:, g * HD : (g + 1) * HD] * fresh, axis=-1, keepdims=True)
            for g in range(2)
        ],
        axis=0,
    )
    own = own * scale

    swapped = pltpu.roll(query, HD, 1)
    low = lax.broadcasted_iota(jnp.int32, query.shape, 1) < HD
    both = jnp.concatenate([jnp.where(low, query, swapped), jnp.where(low, swapped, query)], axis=0)
    both = both * scale
    row_seq = lax.broadcasted_iota(jnp.int32, (2 * pad, 1), 0)
    row_seq = jnp.where(row_seq >= pad, row_seq - pad, row_seq)
    scores = jnp.zeros((2 * pad, span), f32)
    for i, r in enumerate(starts):
        size = min(chunk, total_rows - r)
        parts = [both] * (size // (2 * HD)) + ([both[:, :HD]] if size % (2 * HD) else [])
        left = jnp.concatenate(parts, axis=1) if len(parts) > 1 else parts[0]
        seq = lax.broadcasted_iota(jnp.int32, (1, size), 1) // HD + r // HD
        left = jnp.where(seq == row_seq, left, 0.0).astype(bf16)
        key_copies[i].wait()
        scores = scores + jnp.dot(left, key_buf[r : r + size, :], preferred_element_type=f32)

    limit = jnp.zeros((2 * pad, 1), jnp.int32)
    for b in range(seq_rows):
        limit = jnp.where(row_seq == b, lengths[b], limit)
    position = lax.broadcasted_iota(jnp.int32, (1, span), 1)
    cum = cum_rows[...]
    last = jnp.sum(jnp.where(position == limit - 1, cum, 0.0), axis=-1, keepdims=True)
    scores = jnp.where(position < limit, scores + (last - cum) + log_forget, -jnp.inf)
    top = jnp.maximum(jnp.max(scores, axis=-1, keepdims=True), own)
    expo = jnp.exp(scores - top)
    own_exp = jnp.exp(own - top)
    total = jnp.sum(expo, axis=-1, keepdims=True) + own_exp
    weights = (expo / total).astype(bf16)
    own_weight = (own_exp / total).astype(bf16).astype(f32)

    folded = jnp.zeros((2 * pad, 2 * HD), f32)
    for i, r in enumerate(starts):
        size = min(chunk, total_rows - r)
        value_copies[i].wait()
        wide = lax.dot_general(
            weights, value_buf[r : r + size, :], nt, preferred_element_type=f32
        )
        seq = lax.broadcasted_iota(jnp.int32, (1, size), 1) // HD + r // HD
        wide = jnp.where(seq == row_seq, wide, 0.0)
        for c in range(0, size, 2 * HD):
            piece = wide[:, c : min(c + 2 * HD, size)]
            if piece.shape[1] < 2 * HD:
                piece = jnp.concatenate([piece, jnp.zeros_like(piece)], axis=1)
            folded = folded + piece
    mixed = folded + pltpu.roll(folded, HD, 1)
    mixed = mixed + own_weight * jnp.concatenate(
        [jnp.concatenate([new_values, new_values], axis=1)] * 2, axis=0
    )
    heads = jnp.where(low, mixed[0:pad, :], mixed[pad : 2 * pad, :]).astype(bf16)
    partial = jnp.dot(heads, wo[...], preferred_element_type=f32).astype(bf16)
    blocks = out.shape[0]
    cols = out.shape[2]
    for n in range(blocks):
        out[n] = partial[0:seq_rows, n * cols : (n + 1) * cols]
    for copy in pack_loads:
        copy.wait()


def attention_call(
    tokens,
    gain,
    wq,
    wk,
    wv,
    wf,
    bias,
    wo,
    keys,
    values,
    cumul,
    lengths,
    wg,
    wu,
    wd,
    blocks,
):
    seq_rows, width = tokens.shape
    span = keys.shape[3]
    pad = 16
    chunk = 4 * HD
    count = -(-seq_rows * HD // chunk)
    vmem = pl.BlockSpec(memory_space=pltpu.VMEM)
    smem = pl.BlockSpec(memory_space=pltpu.SMEM)
    hbm = pl.BlockSpec(memory_space=pl.ANY)
    kernel = functools.partial(attention_kernel, seq_rows=seq_rows, pad=pad, chunk=chunk)
    return pl.pallas_call(
        kernel,
        out_shape=(
            pltpu.VMEM((blocks, seq_rows, width // blocks), jnp.bfloat16),
            pltpu.VMEM((3,) + wg.shape, jnp.bfloat16),
        ),
        in_specs=[smem, smem] + [vmem] * 8 + [hbm] * 5,
        out_specs=(vmem, vmem),
        scratch_shapes=[
            pltpu.VMEM((seq_rows * HD, span), jnp.bfloat16),
            pltpu.VMEM((seq_rows * HD, span), jnp.bfloat16),
            pltpu.VMEM((2 * pad, span), jnp.float32),
            pltpu.VMEM((pad, width), jnp.float32),
            pltpu.SemaphoreType.DMA((count,)),
            pltpu.SemaphoreType.DMA((count,)),
            pltpu.SemaphoreType.DMA((2 + width // wg.shape[1],)),
        ],
        name="attention",
    )(
        lengths,
        bias,
        tokens,
        gain.reshape(1, width),
        wq,
        wk.T,
        wv.T,
        wf.T,
        wo,
        cumul,
        keys.reshape(seq_rows * HD, span),
        values.reshape(seq_rows * HD, span),
        wg,
        wu,
        wd,
    )


def expert_kernel(rows, gain, trio, far, out, far_buf, far_sems):
    copies = [
        pltpu.make_async_copy(far.at[i], far_buf.at[i], far_sems.at[i]) for i in range(3)
    ]
    for copy in copies:
        copy.start()
    f32 = jnp.float32
    bf16 = jnp.bfloat16
    blocks, count, cols = rows.shape
    width = gain.shape[1]
    units = trio.shape[2]
    capacity = out.shape[1]
    pieces = [rows[n].astype(f32) for n in range(blocks)]
    squares = sum(jnp.sum(piece * piece, axis=-1, keepdims=True) for piece in pieces)
    inv = lax.rsqrt(squares / width + EPSILON)
    flats = [
        (pieces[n] * inv * gain[:, n * cols : (n + 1) * cols]).astype(bf16) for n in range(blocks)
    ]

    def matrix(pack, i, span):
        if pack == 3:
            return far_buf[i, span, :]
        return trio[3 * pack + i, span, :]

    def projected(pair, i):
        total = 0.0
        for n in range(blocks):
            span = slice(n * cols, (n + 1) * cols)
            weight = jnp.concatenate([matrix(pack, i, span) for pack in pair], axis=1)
            total = total + jnp.dot(flats[n], weight, preferred_element_type=f32)
        return total

    pairs = [(0, 1), (2, 3)]
    hiddens = []
    for pair in pairs:
        if pair[1] == 3:
            for copy in copies:
                copy.wait()
        gate = projected(pair, 0)
        up = projected(pair, 1)
        hiddens.append((gate / (1.0 + jnp.exp(-gate)) * up).astype(bf16))
    for n in range(blocks):
        part = 0.0
        for pair, hidden in zip(pairs, hiddens):
            strips = []
            for j in range(n * cols // units, (n + 1) * cols // units):
                span = slice(j * units, (j + 1) * units)
                strips.append(jnp.concatenate([matrix(pack, 2, span) for pack in pair], axis=0))
            weight = jnp.concatenate(strips, axis=1)
            part = part + jnp.dot(hidden, weight, preferred_element_type=f32)
        slots = count // capacity
        for e in range(slots):
            out[n * slots + e] = part[e * capacity : (e + 1) * capacity, :].astype(bf16)


def expert_call(rows, gain, trio, far, capacity):
    vmem = pl.BlockSpec(memory_space=pltpu.VMEM)
    hbm = pl.BlockSpec(memory_space=pl.ANY)
    blocks, count, cols = rows.shape
    return pl.pallas_call(
        expert_kernel,
        out_shape=pltpu.VMEM((blocks * count // capacity, capacity, cols), jnp.bfloat16),
        in_specs=[vmem, vmem, vmem, hbm],
        out_specs=vmem,
        scratch_shapes=[
            pltpu.VMEM(far.shape, jnp.bfloat16),
            pltpu.SemaphoreType.DMA((3,)),
        ],
        name="expert",
    )(in_vmem(rows), gain.reshape(1, -1), in_vmem(trio), far)


def outgoing_kernel(partials, token_cols, place, out, kept):
    f32 = jnp.float32
    bf16 = jnp.bfloat16
    mixed = sum(partials[n].astype(f32) for n in range(partials.shape[0]))
    residual = (token_cols[...].astype(f32) + mixed).astype(bf16)
    kept[...] = residual
    spread = jnp.dot(place[...], residual, preferred_element_type=f32)
    copies, capacity = out.shape[0], out.shape[1]
    slots = place.shape[0] // capacity
    for e in range(slots):
        rows = spread[e * capacity : (e + 1) * capacity, :].astype(bf16)
        for n in range(copies // slots):
            out[n * slots + e] = rows


def outgoing_call(partials, token_cols, place, capacity):
    vmem = pl.BlockSpec(memory_space=pltpu.VMEM)
    blocks, seq_rows, cols = partials.shape
    total = blocks * place.shape[0] // capacity
    return pl.pallas_call(
        outgoing_kernel,
        out_shape=(
            pltpu.VMEM((total, capacity, cols), jnp.bfloat16),
            pltpu.VMEM((seq_rows, cols), jnp.bfloat16),
        ),
        in_specs=[vmem] * 3,
        out_specs=(vmem, vmem),
        name="outgoing",
    )(in_vmem(partials), in_vmem(token_cols), in_vmem(place))


def in_vmem(array):
    return pltpu.with_memory_space_constraint(array, pltpu.VMEM)


def slot_tables(routes, route_weights, experts, capacity):
    seq_rows = routes.shape[0]
    expert = lax.broadcasted_iota(jnp.int32, (experts, 1, 1), 0)
    chosen = routes[None] == expert
    named = jnp.any(chosen, axis=2).astype(jnp.float32)
    share = jnp.sum(jnp.where(chosen, route_weights[None], 0.0), axis=2)
    first = lax.broadcasted_iota(jnp.int32, (seq_rows, seq_rows), 0)
    second = lax.broadcasted_iota(jnp.int32, (seq_rows, seq_rows), 1)
    earlier = jnp.dot(named, (first < second).astype(jnp.float32))
    slot = lax.broadcasted_iota(jnp.int32, (1, capacity, 1), 1).astype(jnp.float32)
    here = (earlier[:, None, :] == slot) & (named[:, None, :] > 0.0)
    place = here.astype(jnp.bfloat16).reshape(experts * capacity, seq_rows)
    weighted = jnp.where(here, share[:, None, :], 0.0).reshape(experts * capacity, seq_rows)
    return place, weighted.T


def body(
    tokens,
    attn_gain,
    query_weight,
    key_weight,
    value_weight,
    forget_weight,
    forget_bias,
    out_weight,
    key_cache,
    value_cache,
    cum_forget,
    lengths,
    ffn_gain,
    routes,
    route_weights,
    gate_weight,
    up_weight,
    down_weight,
):
    tp_count = lax.axis_size("tp")
    ep_count = lax.axis_size(EXPERT_AXES) * SLICES
    tp_rank = lax.axis_index("tp")
    seq_rows = tokens.shape[0]
    width = tokens.shape[1]
    cols = width // tp_count
    experts = ep_count // SLICES
    capacity = min(seq_rows, max(2, (2 * seq_rows * TOP_K + experts - 1) // experts))
    partial, own_pack = attention_call(
        tokens,
        attn_gain,
        query_weight,
        key_weight,
        value_weight,
        forget_weight,
        forget_bias,
        out_weight,
        key_cache,
        value_cache,
        cum_forget,
        lengths,
        gate_weight[0],
        up_weight[0],
        down_weight[0],
        tp_count,
    )
    blocks = lax.all_to_all(partial, "tp", 0, 0, tiled=True)
    swap = [(0, 1), (1, 0)]
    side_pack = lax.ppermute(own_pack, "xl", swap)
    core_pack = lax.ppermute(own_pack, "core", swap)
    far_pack = lax.ppermute(side_pack, "core", swap)
    trio = jnp.concatenate([own_pack, core_pack, side_pack], axis=0)
    token_cols = lax.dynamic_slice_in_dim(tokens, tp_rank * cols, cols, 1)
    place, weighted = slot_tables(routes, route_weights, experts, capacity)
    outgoing, residual_cols = outgoing_call(blocks, token_cols, place, capacity)
    arrived = whole_exchange(outgoing)
    arrived = arrived.reshape(tp_count, experts * capacity, cols)
    part = expert_call(arrived, ffn_gain, trio, far_pack, capacity)
    parts = whole_exchange(part)
    parts = parts.reshape(tp_count, experts * capacity, cols)
    returned = jnp.sum(parts.astype(jnp.float32), axis=0)
    routed = jnp.dot(
        weighted, returned, precision=lax.Precision.HIGHEST, preferred_element_type=jnp.float32
    )
    return (residual_cols.astype(jnp.float32) + routed).astype(jnp.bfloat16)


def solution(mesh):
    half = mesh.shape["ep"] // (2 * SLICES)
    fine = Mesh(
        mesh.devices.reshape(half, 2, 2, 2, mesh.shape["tp"]), EP_AXES + ("tp",)
    )
    return jax.shard_map(
        body,
        mesh=fine,
        in_specs=(
            P(EP_AXES, None),
            P(),
            P(None, "tp"),
            P(None, "tp"),
            P(None, "tp"),
            P(None, "tp"),
            P("tp"),
            P("tp", None),
            P(EP_AXES, "tp", None, None),
            P(EP_AXES, "tp", None, None),
            P(EP_AXES, "tp", None),
            P(EP_AXES),
            P(),
            P(EP_AXES, None),
            P(EP_AXES, None),
            P(EP_AXES, None, "tp"),
            P(EP_AXES, None, "tp"),
            P(EP_AXES, "tp", None),
        ),
        out_specs=P(EP_AXES, "tp"),
        check_vma=False,
    )
```

```python
import functools

import jax
import jax.numpy as jnp
from jax import lax
from jax.experimental import pallas as pl
from jax.experimental.pallas import tpu as pltpu
from jax.sharding import Mesh
from jax.sharding import PartitionSpec as P


HD = 64
SLICES = 4
TOP_K = 2


EPSILON = 1e-06
EXPERT_AXES = ("z", "xh")
SLICE_AXES = ("xl", "core")
EP_AXES = EXPERT_AXES + SLICE_AXES


def attention_kernel(
    lengths,
    bias,
    tokens_hbm,
    gain_hbm,
    wq_hbm,
    wk_hbm,
    wv_hbm,
    wf_hbm,
    wo_hbm,
    cumul_hbm,
    keys,
    values,
    wg,
    wu,
    wd,
    out,
    pack,
    tokens,
    gain,
    wq,
    wk,
    wv,
    wf,
    wo,
    cumul,
    key_buf,
    value_buf,
    cum_rows,
    token_rows,
    small_sems,
    key_sems,
    value_sems,
    pack_sems,
    *,
    seq_rows,
    pad,
    chunk,
):
    small_copies = [
        pltpu.make_async_copy(source, target, small_sems.at[i])
        for i, (source, target) in enumerate(
            [
                (tokens_hbm, tokens),
                (gain_hbm, gain),
                (wq_hbm, wq),
                (wk_hbm, wk),
                (wv_hbm, wv),
                (wf_hbm, wf),
                (cumul_hbm, cumul),
                (wo_hbm, wo),
            ]
        )
    ]
    for copy in small_copies[:7]:
        copy.start()
    span = keys.shape[1]
    total_rows = seq_rows * HD
    width = tokens.shape[1]
    starts = list(range(0, total_rows, chunk))

    def copies(source, buf, sems):
        return [
            pltpu.make_async_copy(
                source.at[pl.ds(r, min(chunk, total_rows - r))],
                buf.at[pl.ds(r, min(chunk, total_rows - r))],
                sems.at[i],
            )
            for i, r in enumerate(starts)
        ]

    key_copies = copies(keys, key_buf, key_sems)
    value_copies = copies(values, value_buf, value_sems)
    units = wg.shape[1]
    pack_loads = [
        pltpu.make_async_copy(wg, pack.at[0], pack_sems.at[0]),
        pltpu.make_async_copy(wu, pack.at[1], pack_sems.at[1]),
    ] + [
        pltpu.make_async_copy(
            wd.at[:, pl.ds(j * units, units)],
            pack.at[2, pl.ds(j * units, units), :],
            pack_sems.at[2 + j],
        )
        for j in range(wd.shape[1] // units)
    ]
    for copy in key_copies + value_copies + small_copies[7:] + pack_loads:
        copy.start()

    f32 = jnp.float32
    bf16 = jnp.bfloat16
    nt = (((1,), (1,)), ((), ()))
    token_rows[...] = jnp.zeros_like(token_rows)
    cum_rows[...] = jnp.zeros_like(cum_rows)
    for copy in small_copies[:6]:
        copy.wait()
    token_rows[0:seq_rows, :] = tokens[...].astype(f32)

    rows = token_rows[...]
    inv = lax.rsqrt(jnp.sum(rows * rows, axis=-1, keepdims=True) / width + EPSILON)
    normed_f = (rows * inv * gain[...]).astype(bf16).astype(f32)
    normed = normed_f.astype(bf16)
    query = jnp.dot(normed, wq[...], preferred_element_type=f32).astype(bf16).astype(f32)
    fresh = lax.dot_general(normed, wk[...], nt, preferred_element_type=f32)
    fresh = fresh.astype(bf16).astype(f32)
    new_values = lax.dot_general(normed, wv[...], nt, preferred_element_type=f32)
    new_values = new_values.astype(bf16).astype(f32)
    wf_rows = wf[...].astype(f32)
    forget = []
    for g in range(2):
        raw = jnp.sum(normed_f * wf_rows[g : g + 1, :], axis=-1, keepdims=True) + bias[g]
        forget.append(jnp.minimum(raw, 0.0) - jnp.log1p(jnp.exp(-jnp.abs(raw))))
    log_forget = jnp.concatenate(forget, axis=0)

    scale = HD ** (-0.5)
    own = jnp.concatenate(
        [
            jnp.sum(query[:, g * HD : (g + 1) * HD] * fresh, axis=-1, keepdims=True)
            for g in range(2)
        ],
        axis=0,
    )
    own = own * scale

    swapped = pltpu.roll(query, HD, 1)
    low = lax.broadcasted_iota(jnp.int32, query.shape, 1) < HD
    both = jnp.concatenate([jnp.where(low, query, swapped), jnp.where(low, swapped, query)], axis=0)
    both = both * scale
    row_seq = lax.broadcasted_iota(jnp.int32, (2 * pad, 1), 0)
    row_seq = jnp.where(row_seq >= pad, row_seq - pad, row_seq)
    scores = jnp.zeros((2 * pad, span), f32)
    for i, r in enumerate(starts):
        size = min(chunk, total_rows - r)
        parts = [both] * (size // (2 * HD)) + ([both[:, :HD]] if size % (2 * HD) else [])
        left = jnp.concatenate(parts, axis=1) if len(parts) > 1 else parts[0]
        seq = lax.broadcasted_iota(jnp.int32, (1, size), 1) // HD + r // HD
        left = jnp.where(seq == row_seq, left, 0.0).astype(bf16)
        key_copies[i].wait()
        scores = scores + jnp.dot(left, key_buf[r : r + size, :], preferred_element_type=f32)

    small_copies[6].wait()
    for b in range(seq_rows):
        pair = cumul[b]
        cum_rows[b : b + 1, :] = pair[0:1, :]
        cum_rows[pad + b : pad + b + 1, :] = pair[1:2, :]
    limit = jnp.zeros((2 * pad, 1), jnp.int32)
    for b in range(seq_rows):
        limit = jnp.where(row_seq == b, lengths[b], limit)
    position = lax.broadcasted_iota(jnp.int32, (1, span), 1)
    cum = cum_rows[...]
    last = jnp.sum(jnp.where(position == limit - 1, cum, 0.0), axis=-1, keepdims=True)
    scores = jnp.where(position < limit, scores + (last - cum) + log_forget, -jnp.inf)
    top = jnp.maximum(jnp.max(scores, axis=-1, keepdims=True), own)
    expo = jnp.exp(scores - top)
    own_exp = jnp.exp(own - top)
    total = jnp.sum(expo, axis=-1, keepdims=True) + own_exp
    weights = (expo / total).astype(bf16)
    own_weight = (own_exp / total).astype(bf16).astype(f32)

    folded = jnp.zeros((2 * pad, 2 * HD), f32)
    for i, r in enumerate(starts):
        size = min(chunk, total_rows - r)
        value_copies[i].wait()
        wide = lax.dot_general(
            weights, value_buf[r : r + size, :], nt, preferred_element_type=f32
        )
        seq = lax.broadcasted_iota(jnp.int32, (1, size), 1) // HD + r // HD
        wide = jnp.where(seq == row_seq, wide, 0.0)
        for c in range(0, size, 2 * HD):
            piece = wide[:, c : min(c + 2 * HD, size)]
            if piece.shape[1] < 2 * HD:
                piece = jnp.concatenate([piece, jnp.zeros_like(piece)], axis=1)
            folded = folded + piece
    mixed = folded + pltpu.roll(folded, HD, 1)
    mixed = mixed + own_weight * jnp.concatenate(
        [jnp.concatenate([new_values, new_values], axis=1)] * 2, axis=0
    )
    heads = jnp.where(low, mixed[0:pad, :], mixed[pad : 2 * pad, :]).astype(bf16)
    small_copies[7].wait()
    partial = jnp.dot(heads, wo[...], preferred_element_type=f32).astype(bf16)
    for n in range(out.shape[0]):
        out[n] = partial[0:seq_rows, :]
    for copy in pack_loads:
        copy.wait()


def attention_call(
    tokens,
    gain,
    wq,
    wk,
    wv,
    wf,
    bias,
    wo,
    keys,
    values,
    cumul,
    lengths,
    wg,
    wu,
    wd,
    blocks,
):
    seq_rows, width = tokens.shape
    span = keys.shape[3]
    pad = 16
    chunk = 4 * HD
    count = -(-seq_rows * HD // chunk)
    vmem = pl.BlockSpec(memory_space=pltpu.VMEM)
    smem = pl.BlockSpec(memory_space=pltpu.SMEM)
    hbm = pl.BlockSpec(memory_space=pl.ANY)
    kernel = functools.partial(attention_kernel, seq_rows=seq_rows, pad=pad, chunk=chunk)
    return pl.pallas_call(
        kernel,
        out_shape=(
            pltpu.VMEM((blocks, seq_rows, width), jnp.bfloat16),
            pltpu.VMEM((3,) + wg.shape, jnp.bfloat16),
        ),
        in_specs=[smem, smem] + [hbm] * 13,
        out_specs=(vmem, vmem),
        scratch_shapes=[
            pltpu.VMEM(tokens.shape, jnp.bfloat16),
            pltpu.VMEM((1, width), jnp.float32),
            pltpu.VMEM(wq.shape, jnp.bfloat16),
            pltpu.VMEM((HD, width), jnp.bfloat16),
            pltpu.VMEM((HD, width), jnp.bfloat16),
            pltpu.VMEM((2, width), jnp.bfloat16),
            pltpu.VMEM(wo.shape, jnp.bfloat16),
            pltpu.VMEM(cumul.shape, jnp.float32),
            pltpu.VMEM((seq_rows * HD, span), jnp.bfloat16),
            pltpu.VMEM((seq_rows * HD, span), jnp.bfloat16),
            pltpu.VMEM((2 * pad, span), jnp.float32),
            pltpu.VMEM((pad, width), jnp.float32),
            pltpu.SemaphoreType.DMA((8,)),
            pltpu.SemaphoreType.DMA((count,)),
            pltpu.SemaphoreType.DMA((count,)),
            pltpu.SemaphoreType.DMA((2 + width // wg.shape[1],)),
        ],
        name="attention",
    )(
        lengths,
        bias,
        tokens,
        gain.reshape(1, width),
        wq,
        wk.T,
        wv.T,
        wf.T,
        wo,
        cumul,
        keys.reshape(seq_rows * HD, span),
        values.reshape(seq_rows * HD, span),
        wg,
        wu,
        wd,
    )


def expert_kernel(rows, trio, far, out, far_buf, far_sems, *, blocks):
    copies = [
        pltpu.make_async_copy(far.at[i], far_buf.at[i], far_sems.at[i]) for i in range(3)
    ]
    for copy in copies:
        copy.start()
    f32 = jnp.float32
    bf16 = jnp.bfloat16
    count, width = rows.shape
    cols = width // blocks
    units = trio.shape[2]
    capacity = out.shape[1]
    flats = [rows[:, n * cols : (n + 1) * cols] for n in range(blocks)]

    def matrix(pack, i, span):
        if pack == 3:
            return far_buf[i, span, :]
        return trio[3 * pack + i, span, :]

    def projected(pair, i):
        total = 0.0
        for n in range(blocks):
            span = slice(n * cols, (n + 1) * cols)
            weight = jnp.concatenate([matrix(pack, i, span) for pack in pair], axis=1)
            total = total + jnp.dot(flats[n], weight, preferred_element_type=f32)
        return total

    pairs = [(0, 1), (2, 3)]
    hiddens = []
    for pair in pairs:
        if pair[1] == 3:
            for copy in copies:
                copy.wait()
        gate = projected(pair, 0)
        up = projected(pair, 1)
        hiddens.append((gate / (1.0 + jnp.exp(-gate)) * up).astype(bf16))
    for n in range(blocks):
        part = 0.0
        for pair, hidden in zip(pairs, hiddens):
            strips = []
            for j in range(n * cols // units, (n + 1) * cols // units):
                span = slice(j * units, (j + 1) * units)
                strips.append(jnp.concatenate([matrix(pack, 2, span) for pack in pair], axis=0))
            weight = jnp.concatenate(strips, axis=1)
            part = part + jnp.dot(hidden, weight, preferred_element_type=f32)
        slots = count // capacity
        for e in range(slots):
            out[e * blocks + n] = part[e * capacity : (e + 1) * capacity, :].astype(bf16)


def expert_call(rows, trio, far, blocks, capacity):
    vmem = pl.BlockSpec(memory_space=pltpu.VMEM)
    hbm = pl.BlockSpec(memory_space=pl.ANY)
    count, width = rows.shape
    return pl.pallas_call(
        functools.partial(expert_kernel, blocks=blocks),
        out_shape=pltpu.VMEM(
            (blocks * count // capacity, capacity, width // blocks), jnp.bfloat16
        ),
        in_specs=[vmem, vmem, hbm],
        out_specs=vmem,
        scratch_shapes=[
            pltpu.VMEM(far.shape, jnp.bfloat16),
            pltpu.SemaphoreType.DMA((3,)),
        ],
        name="expert",
    )(in_vmem(rows), in_vmem(trio), far)


def outgoing_kernel(partials, tokens, gain, place, out, kept):
    f32 = jnp.float32
    bf16 = jnp.bfloat16
    mixed = sum(partials[n].astype(f32) for n in range(partials.shape[0]))
    residual = (tokens[...].astype(f32) + mixed).astype(bf16)
    kept[...] = residual
    rows = residual.astype(f32)
    inv = lax.rsqrt(jnp.sum(rows * rows, axis=-1, keepdims=True) / rows.shape[1] + EPSILON)
    ffn_in = (rows * inv * gain[...]).astype(bf16)
    spread = jnp.dot(place[...], ffn_in, preferred_element_type=f32)
    capacity = out.shape[1]
    for e in range(out.shape[0]):
        out[e] = spread[e * capacity : (e + 1) * capacity, :].astype(bf16)


def outgoing_call(partials, tokens, gain, place, capacity):
    vmem = pl.BlockSpec(memory_space=pltpu.VMEM)
    _, seq_rows, width = partials.shape
    return pl.pallas_call(
        outgoing_kernel,
        out_shape=(
            pltpu.VMEM((place.shape[0] // capacity, capacity, width), jnp.bfloat16),
            pltpu.VMEM((seq_rows, width), jnp.bfloat16),
        ),
        in_specs=[vmem] * 4,
        out_specs=(vmem, vmem),
        name="outgoing",
    )(in_vmem(partials), in_vmem(tokens), in_vmem(gain.reshape(1, -1)), in_vmem(place))


def in_vmem(array):
    return pltpu.with_memory_space_constraint(array, pltpu.VMEM)


def slot_tables(routes, route_weights, experts, capacity):
    seq_rows = routes.shape[0]
    expert = lax.broadcasted_iota(jnp.int32, (experts, 1, 1), 0)
    chosen = routes[None] == expert
    named = jnp.any(chosen, axis=2).astype(jnp.float32)
    share = jnp.sum(jnp.where(chosen, route_weights[None], 0.0), axis=2)
    first = lax.broadcasted_iota(jnp.int32, (seq_rows, seq_rows), 0)
    second = lax.broadcasted_iota(jnp.int32, (seq_rows, seq_rows), 1)
    earlier = jnp.dot(named, (first < second).astype(jnp.float32))
    slot = lax.broadcasted_iota(jnp.int32, (1, capacity, 1), 1).astype(jnp.float32)
    here = (earlier[:, None, :] == slot) & (named[:, None, :] > 0.0)
    place = here.astype(jnp.bfloat16).reshape(experts * capacity, seq_rows)
    weighted = jnp.where(here, share[:, None, :], 0.0).reshape(experts * capacity, seq_rows)
    return place, weighted.T


def body(
    tokens,
    attn_gain,
    query_weight,
    key_weight,
    value_weight,
    forget_weight,
    forget_bias,
    out_weight,
    key_cache,
    value_cache,
    cum_forget,
    lengths,
    ffn_gain,
    routes,
    route_weights,
    gate_weight,
    up_weight,
    down_weight,
):
    tp_count = lax.axis_size("tp")
    ep_count = lax.axis_size(EXPERT_AXES) * SLICES
    tp_rank = lax.axis_index("tp")
    seq_rows = tokens.shape[0]
    width = tokens.shape[1]
    cols = width // tp_count
    experts = ep_count // SLICES
    capacity = min(seq_rows, max(2, (2 * seq_rows * TOP_K + experts - 1) // experts))
    partial, own_pack = attention_call(
        tokens,
        attn_gain,
        query_weight,
        key_weight,
        value_weight,
        forget_weight,
        forget_bias,
        out_weight,
        key_cache,
        value_cache,
        cum_forget,
        lengths,
        gate_weight[0],
        up_weight[0],
        down_weight[0],
        tp_count,
    )
    blocks = lax.all_to_all(partial, "tp", 0, 0, tiled=True)
    swap = [(0, 1), (1, 0)]
    side_pack = lax.ppermute(own_pack, "xl", swap)
    core_pack = lax.ppermute(own_pack, "core", swap)
    far_pack = lax.ppermute(side_pack, "core", swap)
    trio = jnp.concatenate([own_pack, core_pack, side_pack], axis=0)
    place, weighted = slot_tables(routes, route_weights, experts, capacity)
    outgoing, residual = outgoing_call(blocks, tokens, ffn_gain, place, capacity)
    residual_cols = lax.dynamic_slice_in_dim(residual, tp_rank * cols, cols, 1)
    arrived = lax.all_to_all(outgoing, EXPERT_AXES, split_axis=0, concat_axis=0, tiled=True)
    arrived = arrived.reshape(experts * capacity, width)
    part = expert_call(arrived, trio, far_pack, tp_count, capacity)
    parts = lax.all_to_all(part, EXPERT_AXES + ("tp",), split_axis=0, concat_axis=0, tiled=True)
    parts = parts.reshape(experts, tp_count, capacity, cols)
    returned = jnp.sum(parts.astype(jnp.float32), axis=1).reshape(experts * capacity, cols)
    routed = jnp.dot(
        weighted, returned, precision=lax.Precision.HIGHEST, preferred_element_type=jnp.float32
    )
    return (residual_cols.astype(jnp.float32) + routed).astype(jnp.bfloat16)


def solution(mesh):
    half = mesh.shape["ep"] // (2 * SLICES)
    fine = Mesh(
        mesh.devices.reshape(half, 2, 2, 2, mesh.shape["tp"]), EP_AXES + ("tp",)
    )
    return jax.shard_map(
        body,
        mesh=fine,
        in_specs=(
            P(EP_AXES, None),
            P(),
            P(None, "tp"),
            P(None, "tp"),
            P(None, "tp"),
            P(None, "tp"),
            P("tp"),
            P("tp", None),
            P(EP_AXES, "tp", None, None),
            P(EP_AXES, "tp", None, None),
            P(EP_AXES, "tp", None),
            P(EP_AXES),
            P(),
            P(EP_AXES, None),
            P(EP_AXES, None),
            P(EP_AXES, None, "tp"),
            P(EP_AXES, None, "tp"),
            P(EP_AXES, "tp", None),
        ),
        out_specs=P(EP_AXES, "tp"),
        check_vma=False,
    )
```

```python
import functools

import jax
import jax.numpy as jnp
from jax import lax
from jax.experimental import pallas as pl
from jax.experimental.pallas import tpu as pltpu
from jax.sharding import Mesh
from jax.sharding import PartitionSpec as P


HD = 64
SLICES = 4
TOP_K = 2


EPSILON = 1e-06
EXPERT_AXES = ("z", "xh")
SLICE_AXES = ("xl", "core")
EP_AXES = EXPERT_AXES + SLICE_AXES


def attention_kernel(
    lengths,
    bias,
    tokens_hbm,
    gain_hbm,
    wq_hbm,
    wk_hbm,
    wv_hbm,
    wf_hbm,
    wo_hbm,
    cumul_hbm,
    keys,
    values,
    wg,
    wu,
    wd,
    out,
    pack,
    tokens,
    gain,
    wq,
    wk,
    wv,
    wf,
    wo,
    cumul,
    key_buf,
    value_buf,
    cum_rows,
    token_rows,
    small_sems,
    key_sems,
    value_sems,
    pack_sems,
    *,
    seq_rows,
    pad,
    chunk,
):
    small_copies = [
        pltpu.make_async_copy(source, target, small_sems.at[i])
        for i, (source, target) in enumerate(
            [
                (tokens_hbm, tokens),
                (gain_hbm, gain),
                (wq_hbm, wq),
                (wk_hbm, wk),
                (wv_hbm, wv),
                (wf_hbm, wf),
                (cumul_hbm, cumul),
                (wo_hbm, wo),
            ]
        )
    ]
    for copy in small_copies[:7]:
        copy.start()
    span = keys.shape[1]
    total_rows = seq_rows * HD
    width = tokens.shape[1]
    starts = list(range(0, total_rows, chunk))

    def copies(source, buf, sems):
        return [
            pltpu.make_async_copy(
                source.at[pl.ds(r, min(chunk, total_rows - r))],
                buf.at[pl.ds(r, min(chunk, total_rows - r))],
                sems.at[i],
            )
            for i, r in enumerate(starts)
        ]

    key_copies = copies(keys, key_buf, key_sems)
    value_copies = copies(values, value_buf, value_sems)
    units = wg.shape[1]
    pack_loads = [
        pltpu.make_async_copy(wg, pack.at[0], pack_sems.at[0]),
        pltpu.make_async_copy(wu, pack.at[1], pack_sems.at[1]),
    ] + [
        pltpu.make_async_copy(
            wd.at[:, pl.ds(j * units, units)],
            pack.at[2, pl.ds(j * units, units), :],
            pack_sems.at[2 + j],
        )
        for j in range(wd.shape[1] // units)
    ]
    for copy in key_copies + value_copies + small_copies[7:] + pack_loads:
        copy.start()

    f32 = jnp.float32
    bf16 = jnp.bfloat16
    nt = (((1,), (1,)), ((), ()))
    token_rows[...] = jnp.zeros_like(token_rows)
    cum_rows[...] = jnp.zeros_like(cum_rows)
    for copy in small_copies[:6]:
        copy.wait()
    token_rows[0:seq_rows, :] = tokens[...].astype(f32)

    rows = token_rows[...]
    inv = lax.rsqrt(jnp.sum(rows * rows, axis=-1, keepdims=True) / width + EPSILON)
    normed_f = (rows * inv * gain[...]).astype(bf16).astype(f32)
    normed = normed_f.astype(bf16)
    query = jnp.dot(normed, wq[...], preferred_element_type=f32).astype(bf16).astype(f32)
    fresh = lax.dot_general(normed, wk[...], nt, preferred_element_type=f32)
    fresh = fresh.astype(bf16).astype(f32)
    new_values = lax.dot_general(normed, wv[...], nt, preferred_element_type=f32)
    new_values = new_values.astype(bf16).astype(f32)
    wf_rows = wf[...].astype(f32)
    forget = []
    for g in range(2):
        raw = jnp.sum(normed_f * wf_rows[g : g + 1, :], axis=-1, keepdims=True) + bias[g]
        forget.append(jnp.minimum(raw, 0.0) - jnp.log1p(jnp.exp(-jnp.abs(raw))))
    log_forget = jnp.concatenate(forget, axis=0)

    scale = HD ** (-0.5)
    own = jnp.concatenate(
        [
            jnp.sum(query[:, g * HD : (g + 1) * HD] * fresh, axis=-1, keepdims=True)
            for g in range(2)
        ],
        axis=0,
    )
    own = own * scale

    swapped = pltpu.roll(query, HD, 1)
    low = lax.broadcasted_iota(jnp.int32, query.shape, 1) < HD
    both = jnp.concatenate([jnp.where(low, query, swapped), jnp.where(low, swapped, query)], axis=0)
    both = both * scale
    row_seq = lax.broadcasted_iota(jnp.int32, (2 * pad, 1), 0)
    row_seq = jnp.where(row_seq >= pad, row_seq - pad, row_seq)
    scores = jnp.zeros((2 * pad, span), f32)
    for i, r in enumerate(starts):
        size = min(chunk, total_rows - r)
        parts = [both] * (size // (2 * HD)) + ([both[:, :HD]] if size % (2 * HD) else [])
        left = jnp.concatenate(parts, axis=1) if len(parts) > 1 else parts[0]
        seq = lax.broadcasted_iota(jnp.int32, (1, size), 1) // HD + r // HD
        left = jnp.where(seq == row_seq, left, 0.0).astype(bf16)
        key_copies[i].wait()
        scores = scores + jnp.dot(left, key_buf[r : r + size, :], preferred_element_type=f32)

    small_copies[6].wait()
    for b in range(seq_rows):
        pair = cumul[b]
        cum_rows[b : b + 1, :] = pair[0:1, :]
        cum_rows[pad + b : pad + b + 1, :] = pair[1:2, :]
    limit = jnp.zeros((2 * pad, 1), jnp.int32)
    for b in range(seq_rows):
        limit = jnp.where(row_seq == b, lengths[b], limit)
    position = lax.broadcasted_iota(jnp.int32, (1, span), 1)
    cum = cum_rows[...]
    last = jnp.sum(jnp.where(position == limit - 1, cum, 0.0), axis=-1, keepdims=True)
    scores = jnp.where(position < limit, scores + (last - cum) + log_forget, -jnp.inf)
    top = jnp.maximum(jnp.max(scores, axis=-1, keepdims=True), own)
    expo = jnp.exp(scores - top)
    own_exp = jnp.exp(own - top)
    total = jnp.sum(expo, axis=-1, keepdims=True) + own_exp
    weights = (expo / total).astype(bf16)
    own_weight = (own_exp / total).astype(bf16).astype(f32)

    folded = jnp.zeros((2 * pad, 2 * HD), f32)
    for i, r in enumerate(starts):
        size = min(chunk, total_rows - r)
        value_copies[i].wait()
        wide = lax.dot_general(
            weights, value_buf[r : r + size, :], nt, preferred_element_type=f32
        )
        seq = lax.broadcasted_iota(jnp.int32, (1, size), 1) // HD + r // HD
        wide = jnp.where(seq == row_seq, wide, 0.0)
        for c in range(0, size, 2 * HD):
            piece = wide[:, c : min(c + 2 * HD, size)]
            if piece.shape[1] < 2 * HD:
                piece = jnp.concatenate([piece, jnp.zeros_like(piece)], axis=1)
            folded = folded + piece
    mixed = folded + pltpu.roll(folded, HD, 1)
    mixed = mixed + own_weight * jnp.concatenate(
        [jnp.concatenate([new_values, new_values], axis=1)] * 2, axis=0
    )
    heads = jnp.where(low, mixed[0:pad, :], mixed[pad : 2 * pad, :]).astype(bf16)
    small_copies[7].wait()
    partial = jnp.dot(heads, wo[...], preferred_element_type=f32).astype(bf16)
    for n in range(out.shape[0]):
        out[n] = partial[0:seq_rows, :]
    for copy in pack_loads:
        copy.wait()


def attention_call(
    tokens,
    gain,
    wq,
    wk,
    wv,
    wf,
    bias,
    wo,
    keys,
    values,
    cumul,
    lengths,
    wg,
    wu,
    wd,
    blocks,
):
    seq_rows, width = tokens.shape
    span = keys.shape[3]
    pad = 16
    chunk = 4 * HD
    count = -(-seq_rows * HD // chunk)
    vmem = pl.BlockSpec(memory_space=pltpu.VMEM)
    smem = pl.BlockSpec(memory_space=pltpu.SMEM)
    hbm = pl.BlockSpec(memory_space=pl.ANY)
    kernel = functools.partial(attention_kernel, seq_rows=seq_rows, pad=pad, chunk=chunk)
    return pl.pallas_call(
        kernel,
        out_shape=(
            pltpu.VMEM((blocks, seq_rows, width), jnp.bfloat16),
            pltpu.VMEM((3,) + wg.shape, jnp.bfloat16),
        ),
        in_specs=[smem, smem] + [hbm] * 13,
        out_specs=(vmem, vmem),
        scratch_shapes=[
            pltpu.VMEM(tokens.shape, jnp.bfloat16),
            pltpu.VMEM((1, width), jnp.float32),
            pltpu.VMEM(wq.shape, jnp.bfloat16),
            pltpu.VMEM((HD, width), jnp.bfloat16),
            pltpu.VMEM((HD, width), jnp.bfloat16),
            pltpu.VMEM((2, width), jnp.bfloat16),
            pltpu.VMEM(wo.shape, jnp.bfloat16),
            pltpu.VMEM(cumul.shape, jnp.float32),
            pltpu.VMEM((seq_rows * HD, span), jnp.bfloat16),
            pltpu.VMEM((seq_rows * HD, span), jnp.bfloat16),
            pltpu.VMEM((2 * pad, span), jnp.float32),
            pltpu.VMEM((pad, width), jnp.float32),
            pltpu.SemaphoreType.DMA((8,)),
            pltpu.SemaphoreType.DMA((count,)),
            pltpu.SemaphoreType.DMA((count,)),
            pltpu.SemaphoreType.DMA((2 + width // wg.shape[1],)),
        ],
        name="attention",
    )(
        lengths,
        bias,
        tokens,
        gain.reshape(1, width),
        wq,
        wk.T,
        wv.T,
        wf.T,
        wo,
        cumul,
        keys.reshape(seq_rows * HD, span),
        values.reshape(seq_rows * HD, span),
        wg,
        wu,
        wd,
    )


def expert_kernel(rows, pair, far, out, far_buf, far_sems, *, blocks):
    order = (0, 3, 1, 4, 2, 5)
    copies = {i: pltpu.make_async_copy(far.at[i], far_buf.at[i], far_sems.at[i]) for i in order}
    for i in order:
        copies[i].start()
    f32 = jnp.float32
    bf16 = jnp.bfloat16
    count, width = rows.shape
    cols = width // blocks
    units = pair.shape[2]
    capacity = out.shape[1]
    flats = [rows[:, n * cols : (n + 1) * cols] for n in range(blocks)]

    def projected(packs, i):
        total = 0.0
        for n in range(blocks):
            span = slice(n * cols, (n + 1) * cols)
            weight = jnp.concatenate([packs[i, span, :], packs[3 + i, span, :]], axis=1)
            total = total + jnp.dot(flats[n], weight, preferred_element_type=f32)
        return total

    hiddens = []
    for packs in (pair, far_buf):
        factors = []
        for i in range(2):
            if packs is far_buf:
                copies[i].wait()
                copies[3 + i].wait()
            factors.append(projected(packs, i))
        gate, up = factors
        hiddens.append((gate / (1.0 + jnp.exp(-gate)) * up).astype(bf16))
    copies[2].wait()
    copies[5].wait()
    for n in range(blocks):
        part = 0.0
        for packs, hidden in zip((pair, far_buf), hiddens):
            strips = []
            for j in range(n * cols // units, (n + 1) * cols // units):
                span = slice(j * units, (j + 1) * units)
                strips.append(jnp.concatenate([packs[2, span, :], packs[5, span, :]], axis=0))
            weight = jnp.concatenate(strips, axis=1)
            part = part + jnp.dot(hidden, weight, preferred_element_type=f32)
        slots = count // capacity
        for e in range(slots):
            out[e * blocks + n] = part[e * capacity : (e + 1) * capacity, :].astype(bf16)


def expert_call(rows, pair, far, blocks, capacity):
    vmem = pl.BlockSpec(memory_space=pltpu.VMEM)
    hbm = pl.BlockSpec(memory_space=pl.ANY)
    count, width = rows.shape
    return pl.pallas_call(
        functools.partial(expert_kernel, blocks=blocks),
        out_shape=pltpu.VMEM(
            (blocks * count // capacity, capacity, width // blocks), jnp.bfloat16
        ),
        in_specs=[vmem, vmem, hbm],
        out_specs=vmem,
        scratch_shapes=[
            pltpu.VMEM(far.shape, jnp.bfloat16),
            pltpu.SemaphoreType.DMA((6,)),
        ],
        name="expert",
    )(in_vmem(rows), in_vmem(pair), far)


def outgoing_kernel(partials, tokens, gain, place, out, kept):
    f32 = jnp.float32
    bf16 = jnp.bfloat16
    mixed = sum(partials[n].astype(f32) for n in range(partials.shape[0]))
    residual = (tokens[...].astype(f32) + mixed).astype(bf16)
    kept[...] = residual
    rows = residual.astype(f32)
    inv = lax.rsqrt(jnp.sum(rows * rows, axis=-1, keepdims=True) / rows.shape[1] + EPSILON)
    ffn_in = (rows * inv * gain[...]).astype(bf16)
    spread = jnp.dot(place[...], ffn_in, preferred_element_type=f32)
    capacity = out.shape[1]
    for e in range(out.shape[0]):
        out[e] = spread[e * capacity : (e + 1) * capacity, :].astype(bf16)


def outgoing_call(partials, tokens, gain, place, capacity):
    vmem = pl.BlockSpec(memory_space=pltpu.VMEM)
    _, seq_rows, width = partials.shape
    return pl.pallas_call(
        outgoing_kernel,
        out_shape=(
            pltpu.VMEM((place.shape[0] // capacity, capacity, width), jnp.bfloat16),
            pltpu.VMEM((seq_rows, width), jnp.bfloat16),
        ),
        in_specs=[vmem] * 4,
        out_specs=(vmem, vmem),
        name="outgoing",
    )(in_vmem(partials), in_vmem(tokens), in_vmem(gain.reshape(1, -1)), in_vmem(place))


def in_vmem(array):
    return pltpu.with_memory_space_constraint(array, pltpu.VMEM)


def slot_tables(routes, route_weights, experts, capacity):
    seq_rows = routes.shape[0]
    expert = lax.broadcasted_iota(jnp.int32, (experts, 1, 1), 0)
    chosen = routes[None] == expert
    named = jnp.any(chosen, axis=2).astype(jnp.float32)
    share = jnp.sum(jnp.where(chosen, route_weights[None], 0.0), axis=2)
    first = lax.broadcasted_iota(jnp.int32, (seq_rows, seq_rows), 0)
    second = lax.broadcasted_iota(jnp.int32, (seq_rows, seq_rows), 1)
    earlier = jnp.dot(named, (first < second).astype(jnp.float32))
    slot = lax.broadcasted_iota(jnp.int32, (1, capacity, 1), 1).astype(jnp.float32)
    here = (earlier[:, None, :] == slot) & (named[:, None, :] > 0.0)
    place = here.astype(jnp.bfloat16).reshape(experts * capacity, seq_rows)
    weighted = jnp.where(here, share[:, None, :], 0.0).reshape(experts * capacity, seq_rows)
    return place, weighted.T


def body(
    tokens,
    attn_gain,
    query_weight,
    key_weight,
    value_weight,
    forget_weight,
    forget_bias,
    out_weight,
    key_cache,
    value_cache,
    cum_forget,
    lengths,
    ffn_gain,
    routes,
    route_weights,
    gate_weight,
    up_weight,
    down_weight,
):
    tp_count = lax.axis_size("tp")
    ep_count = lax.axis_size(EXPERT_AXES) * SLICES
    tp_rank = lax.axis_index("tp")
    seq_rows = tokens.shape[0]
    width = tokens.shape[1]
    cols = width // tp_count
    experts = ep_count // SLICES
    capacity = min(seq_rows, max(2, (2 * seq_rows * TOP_K + experts - 1) // experts))
    partial, own_pack = attention_call(
        tokens,
        attn_gain,
        query_weight,
        key_weight,
        value_weight,
        forget_weight,
        forget_bias,
        out_weight,
        key_cache,
        value_cache,
        cum_forget,
        lengths,
        gate_weight[0],
        up_weight[0],
        down_weight[0],
        tp_count,
    )
    blocks = lax.all_to_all(partial, "tp", 0, 0, tiled=True)
    swap = [(0, 1), (1, 0)]
    side_pack = lax.ppermute(own_pack, "xl", swap)
    pair = jnp.concatenate([own_pack, side_pack], axis=0)
    far_pair = lax.ppermute(pair, "core", swap)
    place, weighted = slot_tables(routes, route_weights, experts, capacity)
    outgoing, residual = outgoing_call(blocks, tokens, ffn_gain, place, capacity)
    residual_cols = lax.dynamic_slice_in_dim(residual, tp_rank * cols, cols, 1)
    arrived = lax.all_to_all(outgoing, EXPERT_AXES, split_axis=0, concat_axis=0, tiled=True)
    arrived = arrived.reshape(experts * capacity, width)
    part = expert_call(arrived, pair, far_pair, tp_count, capacity)
    parts = lax.all_to_all(part, EXPERT_AXES + ("tp",), split_axis=0, concat_axis=0, tiled=True)
    parts = parts.reshape(experts, tp_count, capacity, cols)
    returned = jnp.sum(parts.astype(jnp.float32), axis=1).reshape(experts * capacity, cols)
    routed = jnp.dot(
        weighted, returned, precision=lax.Precision.HIGHEST, preferred_element_type=jnp.float32
    )
    return (residual_cols.astype(jnp.float32) + routed).astype(jnp.bfloat16)


def solution(mesh):
    half = mesh.shape["ep"] // (2 * SLICES)
    fine = Mesh(
        mesh.devices.reshape(half, 2, 2, 2, mesh.shape["tp"]), EP_AXES + ("tp",)
    )
    return jax.shard_map(
        body,
        mesh=fine,
        in_specs=(
            P(EP_AXES, None),
            P(),
            P(None, "tp"),
            P(None, "tp"),
            P(None, "tp"),
            P(None, "tp"),
            P("tp"),
            P("tp", None),
            P(EP_AXES, "tp", None, None),
            P(EP_AXES, "tp", None, None),
            P(EP_AXES, "tp", None),
            P(EP_AXES),
            P(),
            P(EP_AXES, None),
            P(EP_AXES, None),
            P(EP_AXES, None, "tp"),
            P(EP_AXES, None, "tp"),
            P(EP_AXES, "tp", None),
        ),
        out_specs=P(EP_AXES, "tp"),
        check_vma=False,
    )
```

```python
import functools

import jax
import jax.numpy as jnp
from jax import lax
from jax.experimental import pallas as pl
from jax.experimental.pallas import tpu as pltpu
from jax.sharding import Mesh
from jax.sharding import PartitionSpec as P


HD = 64
SLICES = 4
TOP_K = 2


EPSILON = 1e-06
EXPERT_AXES = ("z", "xh")
SLICE_AXES = ("xl", "core")
EP_AXES = EXPERT_AXES + SLICE_AXES


def attention_kernel(
    lengths_hbm,
    bias_hbm,
    tokens_hbm,
    gain_hbm,
    wq_hbm,
    wk_hbm,
    wv_hbm,
    wf_hbm,
    wo_hbm,
    cumul_hbm,
    keys,
    values,
    wg,
    wu,
    wd,
    out,
    pack,
    lengths,
    bias,
    tokens,
    gain,
    wq,
    wk,
    wv,
    wf,
    wo,
    cumul,
    key_buf,
    value_buf,
    cum_rows,
    token_rows,
    small_sems,
    key_sems,
    value_sems,
    pack_sems,
    *,
    seq_rows,
    pad,
    chunk,
):
    small_copies = [
        pltpu.make_async_copy(source, target, small_sems.at[i])
        for i, (source, target) in enumerate(
            [
                (tokens_hbm, tokens),
                (gain_hbm, gain),
                (wq_hbm, wq),
                (wk_hbm, wk),
                (wv_hbm, wv),
                (wf_hbm, wf),
                (cumul_hbm, cumul),
                (wo_hbm, wo),
                (lengths_hbm, lengths),
                (bias_hbm, bias),
            ]
        )
    ]
    for copy in small_copies[:7] + small_copies[8:]:
        copy.start()
    span = keys.shape[1]
    total_rows = seq_rows * HD
    width = tokens.shape[1]
    starts = list(range(0, total_rows, chunk))

    def copies(source, buf, sems):
        return [
            pltpu.make_async_copy(
                source.at[pl.ds(r, min(chunk, total_rows - r))],
                buf.at[pl.ds(r, min(chunk, total_rows - r))],
                sems.at[i],
            )
            for i, r in enumerate(starts)
        ]

    key_copies = copies(keys, key_buf, key_sems)
    value_copies = copies(values, value_buf, value_sems)
    units = wg.shape[1]
    pack_loads = [
        pltpu.make_async_copy(wg, pack.at[0], pack_sems.at[0]),
        pltpu.make_async_copy(wu, pack.at[1], pack_sems.at[1]),
    ] + [
        pltpu.make_async_copy(
            wd.at[:, pl.ds(j * units, units)],
            pack.at[2, pl.ds(j * units, units), :],
            pack_sems.at[2 + j],
        )
        for j in range(wd.shape[1] // units)
    ]
    for copy in key_copies + value_copies + small_copies[7:8]:
        copy.start()

    f32 = jnp.float32
    bf16 = jnp.bfloat16
    nt = (((1,), (1,)), ((), ()))
    token_rows[...] = jnp.zeros_like(token_rows)
    cum_rows[...] = jnp.zeros_like(cum_rows)
    for copy in small_copies[:6] + small_copies[8:]:
        copy.wait()
    token_rows[0:seq_rows, :] = tokens[...].astype(f32)

    rows = token_rows[...]
    inv = lax.rsqrt(jnp.sum(rows * rows, axis=-1, keepdims=True) / width + EPSILON)
    normed_f = (rows * inv * gain[...]).astype(bf16).astype(f32)
    normed = normed_f.astype(bf16)
    query = jnp.dot(normed, wq[...], preferred_element_type=f32).astype(bf16).astype(f32)
    fresh = lax.dot_general(normed, wk[...], nt, preferred_element_type=f32)
    fresh = fresh.astype(bf16).astype(f32)
    new_values = lax.dot_general(normed, wv[...], nt, preferred_element_type=f32)
    new_values = new_values.astype(bf16).astype(f32)
    wf_rows = wf[...].astype(f32)
    forget = []
    for g in range(2):
        raw = jnp.sum(normed_f * wf_rows[g : g + 1, :], axis=-1, keepdims=True) + bias[:, g : g + 1]
        forget.append(jnp.minimum(raw, 0.0) - jnp.log1p(jnp.exp(-jnp.abs(raw))))
    log_forget = jnp.concatenate(forget, axis=0)

    scale = HD ** (-0.5)
    own = jnp.concatenate(
        [
            jnp.sum(query[:, g * HD : (g + 1) * HD] * fresh, axis=-1, keepdims=True)
            for g in range(2)
        ],
        axis=0,
    )
    own = own * scale

    swapped = pltpu.roll(query, HD, 1)
    low = lax.broadcasted_iota(jnp.int32, query.shape, 1) < HD
    both = jnp.concatenate([jnp.where(low, query, swapped), jnp.where(low, swapped, query)], axis=0)
    both = both * scale
    row_seq = lax.broadcasted_iota(jnp.int32, (2 * pad, 1), 0)
    row_seq = jnp.where(row_seq >= pad, row_seq - pad, row_seq)
    scores = jnp.zeros((2 * pad, span), f32)
    for i, r in enumerate(starts):
        size = min(chunk, total_rows - r)
        parts = [both] * (size // (2 * HD)) + ([both[:, :HD]] if size % (2 * HD) else [])
        left = jnp.concatenate(parts, axis=1) if len(parts) > 1 else parts[0]
        seq = lax.broadcasted_iota(jnp.int32, (1, size), 1) // HD + r // HD
        left = jnp.where(seq == row_seq, left, 0.0).astype(bf16)
        key_copies[i].wait()
        scores = scores + jnp.dot(left, key_buf[r : r + size, :], preferred_element_type=f32)

    for copy in pack_loads:
        copy.start()
    small_copies[6].wait()
    for b in range(seq_rows):
        pair = cumul[b]
        cum_rows[b : b + 1, :] = pair[0:1, :]
        cum_rows[pad + b : pad + b + 1, :] = pair[1:2, :]
    seq_lane = lax.broadcasted_iota(jnp.int32, (1, seq_rows), 1)
    counts = lengths[...].astype(f32)
    limit = jnp.sum(jnp.where(seq_lane == row_seq, counts, 0.0), axis=-1, keepdims=True)
    limit = limit.astype(jnp.int32)
    position = lax.broadcasted_iota(jnp.int32, (1, span), 1)
    cum = cum_rows[...]
    last = jnp.sum(jnp.where(position == limit - 1, cum, 0.0), axis=-1, keepdims=True)
    scores = jnp.where(position < limit, scores + (last - cum) + log_forget, -jnp.inf)
    top = jnp.maximum(jnp.max(scores, axis=-1, keepdims=True), own)
    expo = jnp.exp(scores - top)
    own_exp = jnp.exp(own - top)
    total = jnp.sum(expo, axis=-1, keepdims=True) + own_exp
    weights = (expo / total).astype(bf16)
    own_weight = (own_exp / total).astype(bf16).astype(f32)

    folded = jnp.zeros((2 * pad, 2 * HD), f32)
    for i, r in enumerate(starts):
        size = min(chunk, total_rows - r)
        value_copies[i].wait()
        wide = lax.dot_general(
            weights, value_buf[r : r + size, :], nt, preferred_element_type=f32
        )
        seq = lax.broadcasted_iota(jnp.int32, (1, size), 1) // HD + r // HD
        wide = jnp.where(seq == row_seq, wide, 0.0)
        for c in range(0, size, 2 * HD):
            piece = wide[:, c : min(c + 2 * HD, size)]
            if piece.shape[1] < 2 * HD:
                piece = jnp.concatenate([piece, jnp.zeros_like(piece)], axis=1)
            folded = folded + piece
    mixed = folded + pltpu.roll(folded, HD, 1)
    mixed = mixed + own_weight * jnp.concatenate(
        [jnp.concatenate([new_values, new_values], axis=1)] * 2, axis=0
    )
    heads = jnp.where(low, mixed[0:pad, :], mixed[pad : 2 * pad, :]).astype(bf16)
    small_copies[7].wait()
    partial = jnp.dot(heads, wo[...], preferred_element_type=f32).astype(bf16)
    for n in range(out.shape[0]):
        out[n] = partial[0:seq_rows, :]
    for copy in pack_loads:
        copy.wait()


def attention_call(
    tokens,
    gain,
    wq,
    wk,
    wv,
    wf,
    bias,
    wo,
    keys,
    values,
    cumul,
    lengths,
    wg,
    wu,
    wd,
    blocks,
):
    seq_rows, width = tokens.shape
    span = keys.shape[3]
    pad = 16
    chunk = 2 * HD * -(-seq_rows // 2)
    count = -(-seq_rows * HD // chunk)
    vmem = pl.BlockSpec(memory_space=pltpu.VMEM)
    hbm = pl.BlockSpec(memory_space=pl.ANY)
    kernel = functools.partial(attention_kernel, seq_rows=seq_rows, pad=pad, chunk=chunk)
    return pl.pallas_call(
        kernel,
        out_shape=(
            pltpu.VMEM((blocks, seq_rows, width), jnp.bfloat16),
            pltpu.VMEM((3,) + wg.shape, jnp.bfloat16),
        ),
        in_specs=[hbm] * 15,
        out_specs=(vmem, vmem),
        scratch_shapes=[
            pltpu.VMEM((1, seq_rows), jnp.int32),
            pltpu.VMEM((1, bias.shape[0]), jnp.float32),
            pltpu.VMEM(tokens.shape, jnp.bfloat16),
            pltpu.VMEM((1, width), jnp.float32),
            pltpu.VMEM(wq.shape, jnp.bfloat16),
            pltpu.VMEM((HD, width), jnp.bfloat16),
            pltpu.VMEM((HD, width), jnp.bfloat16),
            pltpu.VMEM((2, width), jnp.bfloat16),
            pltpu.VMEM(wo.shape, jnp.bfloat16),
            pltpu.VMEM(cumul.shape, jnp.float32),
            pltpu.VMEM((seq_rows * HD, span), jnp.bfloat16),
            pltpu.VMEM((seq_rows * HD, span), jnp.bfloat16),
            pltpu.VMEM((2 * pad, span), jnp.float32),
            pltpu.VMEM((pad, width), jnp.float32),
            pltpu.SemaphoreType.DMA((10,)),
            pltpu.SemaphoreType.DMA((count,)),
            pltpu.SemaphoreType.DMA((count,)),
            pltpu.SemaphoreType.DMA((2 + width // wg.shape[1],)),
        ],
        name="attention",
    )(
        lengths.reshape(1, seq_rows),
        bias.reshape(1, -1),
        tokens,
        gain.reshape(1, width),
        wq,
        wk.T,
        wv.T,
        wf.T,
        wo,
        cumul,
        keys.reshape(seq_rows * HD, span),
        values.reshape(seq_rows * HD, span),
        wg,
        wu,
        wd,
    )


def expert_kernel(rows, trio, far, out, far_buf, far_sems, *, blocks):
    copies = [
        pltpu.make_async_copy(far.at[i], far_buf.at[i], far_sems.at[i]) for i in range(3)
    ]
    for copy in copies:
        copy.start()
    f32 = jnp.float32
    bf16 = jnp.bfloat16
    count, width = rows.shape
    cols = width // blocks
    units = trio.shape[2]
    capacity = out.shape[1]
    flats = [rows[:, n * cols : (n + 1) * cols] for n in range(blocks)]

    def matrix(pack, i, span):
        if pack == 3:
            return far_buf[i, span, :]
        return trio[3 * pack + i, span, :]

    def projected(pair, i):
        total = 0.0
        for n in range(blocks):
            span = slice(n * cols, (n + 1) * cols)
            weight = jnp.concatenate([matrix(pack, i, span) for pack in pair], axis=1)
            total = total + jnp.dot(flats[n], weight, preferred_element_type=f32)
        return total

    pairs = [(0, 1), (2, 3)]
    hiddens = []
    for pair in pairs:
        if pair[1] == 3:
            for copy in copies:
                copy.wait()
        gate = projected(pair, 0)
        up = projected(pair, 1)
        hiddens.append((gate / (1.0 + jnp.exp(-gate)) * up).astype(bf16))
    for n in range(blocks):
        part = 0.0
        for pair, hidden in zip(pairs, hiddens):
            strips = []
            for j in range(n * cols // units, (n + 1) * cols // units):
                span = slice(j * units, (j + 1) * units)
                strips.append(jnp.concatenate([matrix(pack, 2, span) for pack in pair], axis=0))
            weight = jnp.concatenate(strips, axis=1)
            part = part + jnp.dot(hidden, weight, preferred_element_type=f32)
        slots = count // capacity
        for e in range(slots):
            out[e * blocks + n] = part[e * capacity : (e + 1) * capacity, :].astype(bf16)


def expert_call(rows, trio, far, blocks, capacity):
    vmem = pl.BlockSpec(memory_space=pltpu.VMEM)
    hbm = pl.BlockSpec(memory_space=pl.ANY)
    count, width = rows.shape
    return pl.pallas_call(
        functools.partial(expert_kernel, blocks=blocks),
        out_shape=pltpu.VMEM(
            (blocks * count // capacity, capacity, width // blocks), jnp.bfloat16
        ),
        in_specs=[vmem, vmem, hbm],
        out_specs=vmem,
        scratch_shapes=[
            pltpu.VMEM(far.shape, jnp.bfloat16),
            pltpu.SemaphoreType.DMA((3,)),
        ],
        name="expert",
    )(in_vmem(rows), in_vmem(trio), far)


def outgoing_kernel(partials, tokens, gain, place, out, kept):
    f32 = jnp.float32
    bf16 = jnp.bfloat16
    mixed = sum(partials[n].astype(f32) for n in range(partials.shape[0]))
    residual = (tokens[...].astype(f32) + mixed).astype(bf16)
    kept[...] = residual
    rows = residual.astype(f32)
    inv = lax.rsqrt(jnp.sum(rows * rows, axis=-1, keepdims=True) / rows.shape[1] + EPSILON)
    ffn_in = (rows * inv * gain[...]).astype(bf16)
    spread = jnp.dot(place[...], ffn_in, preferred_element_type=f32)
    capacity = out.shape[1]
    for e in range(out.shape[0]):
        out[e] = spread[e * capacity : (e + 1) * capacity, :].astype(bf16)


def outgoing_call(partials, tokens, gain, place, capacity):
    vmem = pl.BlockSpec(memory_space=pltpu.VMEM)
    _, seq_rows, width = partials.shape
    return pl.pallas_call(
        outgoing_kernel,
        out_shape=(
            pltpu.VMEM((place.shape[0] // capacity, capacity, width), jnp.bfloat16),
            pltpu.VMEM((seq_rows, width), jnp.bfloat16),
        ),
        in_specs=[vmem] * 4,
        out_specs=(vmem, vmem),
        name="outgoing",
    )(in_vmem(partials), in_vmem(tokens), in_vmem(gain.reshape(1, -1)), in_vmem(place))


def in_vmem(array):
    return pltpu.with_memory_space_constraint(array, pltpu.VMEM)


def slot_tables(routes, route_weights, experts, capacity):
    seq_rows = routes.shape[0]
    expert = lax.broadcasted_iota(jnp.int32, (experts, 1, 1), 0)
    chosen = routes[None] == expert
    named = jnp.any(chosen, axis=2).astype(jnp.float32)
    share = jnp.sum(jnp.where(chosen, route_weights[None], 0.0), axis=2)
    first = lax.broadcasted_iota(jnp.int32, (seq_rows, seq_rows), 0)
    second = lax.broadcasted_iota(jnp.int32, (seq_rows, seq_rows), 1)
    earlier = jnp.dot(named, (first < second).astype(jnp.float32))
    slot = lax.broadcasted_iota(jnp.int32, (1, capacity, 1), 1).astype(jnp.float32)
    here = (earlier[:, None, :] == slot) & (named[:, None, :] > 0.0)
    place = here.astype(jnp.bfloat16).reshape(experts * capacity, seq_rows)
    weighted = jnp.where(here, share[:, None, :], 0.0).reshape(experts * capacity, seq_rows)
    return place, weighted.T


def body(
    tokens,
    attn_gain,
    query_weight,
    key_weight,
    value_weight,
    forget_weight,
    forget_bias,
    out_weight,
    key_cache,
    value_cache,
    cum_forget,
    lengths,
    ffn_gain,
    routes,
    route_weights,
    gate_weight,
    up_weight,
    down_weight,
):
    tp_count = lax.axis_size("tp")
    ep_count = lax.axis_size(EXPERT_AXES) * SLICES
    tp_rank = lax.axis_index("tp")
    seq_rows = tokens.shape[0]
    width = tokens.shape[1]
    cols = width // tp_count
    experts = ep_count // SLICES
    capacity = min(seq_rows, max(2, (2 * seq_rows * TOP_K + experts - 1) // experts))
    partial, own_pack = attention_call(
        tokens,
        attn_gain,
        query_weight,
        key_weight,
        value_weight,
        forget_weight,
        forget_bias,
        out_weight,
        key_cache,
        value_cache,
        cum_forget,
        lengths,
        gate_weight[0],
        up_weight[0],
        down_weight[0],
        tp_count,
    )
    blocks = lax.all_to_all(partial, "tp", 0, 0, tiled=True)
    swap = [(0, 1), (1, 0)]
    side_pack = lax.ppermute(own_pack, "xl", swap)
    core_pack = lax.ppermute(own_pack, "core", swap)
    far_pack = lax.ppermute(side_pack, "core", swap)
    trio = jnp.concatenate([own_pack, core_pack, side_pack], axis=0)
    place, weighted = slot_tables(routes, route_weights, experts, capacity)
    outgoing, residual = outgoing_call(blocks, tokens, ffn_gain, place, capacity)
    residual_cols = lax.dynamic_slice_in_dim(residual, tp_rank * cols, cols, 1)
    arrived = lax.all_to_all(outgoing, EXPERT_AXES, split_axis=0, concat_axis=0, tiled=True)
    arrived = arrived.reshape(experts * capacity, width)
    part = expert_call(arrived, trio, far_pack, tp_count, capacity)
    parts = lax.all_to_all(part, EXPERT_AXES + ("tp",), split_axis=0, concat_axis=0, tiled=True)
    parts = parts.reshape(experts, tp_count, capacity, cols)
    returned = jnp.sum(parts.astype(jnp.float32), axis=1).reshape(experts * capacity, cols)
    routed = jnp.dot(
        weighted, returned, precision=lax.Precision.HIGHEST, preferred_element_type=jnp.float32
    )
    return (residual_cols.astype(jnp.float32) + routed).astype(jnp.bfloat16)


def solution(mesh):
    half = mesh.shape["ep"] // (2 * SLICES)
    fine = Mesh(
        mesh.devices.reshape(half, 2, 2, 2, mesh.shape["tp"]), EP_AXES + ("tp",)
    )
    return jax.shard_map(
        body,
        mesh=fine,
        in_specs=(
            P(EP_AXES, None),
            P(),
            P(None, "tp"),
            P(None, "tp"),
            P(None, "tp"),
            P(None, "tp"),
            P("tp"),
            P("tp", None),
            P(EP_AXES, "tp", None, None),
            P(EP_AXES, "tp", None, None),
            P(EP_AXES, "tp", None),
            P(EP_AXES),
            P(),
            P(EP_AXES, None),
            P(EP_AXES, None),
            P(EP_AXES, None, "tp"),
            P(EP_AXES, None, "tp"),
            P(EP_AXES, "tp", None),
        ),
        out_specs=P(EP_AXES, "tp"),
        check_vma=False,
    )
```

```python
import functools

import jax
import jax.numpy as jnp
from jax import lax
from jax.experimental import pallas as pl
from jax.experimental.pallas import tpu as pltpu
from jax.sharding import Mesh
from jax.sharding import PartitionSpec as P


HD = 64
SLICES = 4
TOP_K = 2


EPSILON = 1e-06
EXPERT_AXES = ("z", "xh")
SLICE_AXES = ("xl", "core")
EP_AXES = EXPERT_AXES + SLICE_AXES


def attention_kernel(
    lengths_hbm,
    bias_hbm,
    tokens_hbm,
    gain_hbm,
    wq_hbm,
    wk_hbm,
    wv_hbm,
    wf_hbm,
    wo_hbm,
    cumul_hbm,
    keys,
    values,
    wg,
    wu,
    wd,
    routes_hbm,
    shares_hbm,
    out,
    pack,
    place,
    weighted,
    routes,
    shares,
    lengths,
    bias,
    tokens,
    gain,
    wq,
    wk,
    wv,
    wf,
    wo,
    cumul,
    key_buf,
    value_buf,
    cum_rows,
    token_rows,
    small_sems,
    key_sems,
    value_sems,
    pack_sems,
    *,
    seq_rows,
    pad,
    chunk,
    capacity,
):
    small_copies = [
        pltpu.make_async_copy(source, target, small_sems.at[i])
        for i, (source, target) in enumerate(
            [
                (tokens_hbm, tokens),
                (gain_hbm, gain),
                (wq_hbm, wq),
                (wk_hbm, wk),
                (wv_hbm, wv),
                (wf_hbm, wf),
                (cumul_hbm, cumul),
                (wo_hbm, wo),
                (lengths_hbm, lengths),
                (bias_hbm, bias),
                (routes_hbm, routes),
                (shares_hbm, shares),
            ]
        )
    ]
    for copy in small_copies[:7] + small_copies[8:]:
        copy.start()
    span = keys.shape[1]
    total_rows = seq_rows * HD
    width = tokens.shape[1]
    starts = list(range(0, total_rows, chunk))

    def copies(source, buf, sems):
        return [
            pltpu.make_async_copy(
                source.at[pl.ds(r, min(chunk, total_rows - r))],
                buf.at[pl.ds(r, min(chunk, total_rows - r))],
                sems.at[i],
            )
            for i, r in enumerate(starts)
        ]

    key_copies = copies(keys, key_buf, key_sems)
    value_copies = copies(values, value_buf, value_sems)
    units = wg.shape[1]
    pack_loads = [
        pltpu.make_async_copy(wg, pack.at[0], pack_sems.at[0]),
        pltpu.make_async_copy(wu, pack.at[1], pack_sems.at[1]),
    ] + [
        pltpu.make_async_copy(
            wd.at[:, pl.ds(j * units, units)],
            pack.at[2, pl.ds(j * units, units), :],
            pack_sems.at[2 + j],
        )
        for j in range(wd.shape[1] // units)
    ]
    for copy in key_copies + value_copies + small_copies[7:8]:
        copy.start()

    f32 = jnp.float32
    bf16 = jnp.bfloat16
    nt = (((1,), (1,)), ((), ()))
    token_rows[...] = jnp.zeros_like(token_rows)
    cum_rows[...] = jnp.zeros_like(cum_rows)
    for copy in small_copies[:2]:
        copy.wait()
    token_rows[0:seq_rows, :] = tokens[...].astype(f32)

    rows = token_rows[...]
    inv = lax.rsqrt(jnp.sum(rows * rows, axis=-1, keepdims=True) / width + EPSILON)
    normed_f = (rows * inv * gain[...]).astype(bf16).astype(f32)
    normed = normed_f.astype(bf16)
    for copy in small_copies[2:6] + small_copies[8:]:
        copy.wait()
    query = jnp.dot(normed, wq[...], preferred_element_type=f32).astype(bf16).astype(f32)
    fresh = lax.dot_general(normed, wk[...], nt, preferred_element_type=f32)
    fresh = fresh.astype(bf16).astype(f32)
    new_values = lax.dot_general(normed, wv[...], nt, preferred_element_type=f32)
    new_values = new_values.astype(bf16).astype(f32)
    wf_rows = wf[...].astype(f32)
    forget = []
    for g in range(2):
        raw = jnp.sum(normed_f * wf_rows[g : g + 1, :], axis=-1, keepdims=True) + bias[:, g : g + 1]
        forget.append(jnp.minimum(raw, 0.0) - jnp.log1p(jnp.exp(-jnp.abs(raw))))
    log_forget = jnp.concatenate(forget, axis=0)

    scale = HD ** (-0.5)
    own = jnp.concatenate(
        [
            jnp.sum(query[:, g * HD : (g + 1) * HD] * fresh, axis=-1, keepdims=True)
            for g in range(2)
        ],
        axis=0,
    )
    own = own * scale

    swapped = pltpu.roll(query, HD, 1)
    low = lax.broadcasted_iota(jnp.int32, query.shape, 1) < HD
    both = jnp.concatenate([jnp.where(low, query, swapped), jnp.where(low, swapped, query)], axis=0)
    both = both * scale
    row_seq = lax.broadcasted_iota(jnp.int32, (2 * pad, 1), 0)
    row_seq = jnp.where(row_seq >= pad, row_seq - pad, row_seq)
    scores = jnp.zeros((2 * pad, span), f32)
    for i, r in enumerate(starts):
        size = min(chunk, total_rows - r)
        parts = [both] * (size // (2 * HD)) + ([both[:, :HD]] if size % (2 * HD) else [])
        left = jnp.concatenate(parts, axis=1) if len(parts) > 1 else parts[0]
        seq = lax.broadcasted_iota(jnp.int32, (1, size), 1) // HD + r // HD
        left = jnp.where(seq == row_seq, left, 0.0).astype(bf16)
        key_copies[i].wait()
        scores = scores + jnp.dot(left, key_buf[r : r + size, :], preferred_element_type=f32)

    for copy in pack_loads:
        copy.start()
    slot = lax.broadcasted_iota(jnp.int32, (place.shape[0], 1), 0)
    expert = slot // capacity
    chosen = [routes[k : k + 1, :] == expert for k in range(TOP_K)]
    named = sum(jnp.where(hit, 1.0, 0.0) for hit in chosen)
    first = lax.broadcasted_iota(jnp.int32, (seq_rows, seq_rows), 0)
    second = lax.broadcasted_iota(jnp.int32, (seq_rows, seq_rows), 1)
    before = jnp.where(first < second, 1.0, 0.0).astype(bf16)
    earlier = jnp.dot(named.astype(bf16), before, preferred_element_type=f32)
    here = jnp.where(earlier == (slot - expert * capacity).astype(f32), named, 0.0)
    share = sum(jnp.where(chosen[k], shares[k : k + 1, :], 0.0) for k in range(TOP_K))
    place[...] = here.astype(bf16)
    weighted[...] = here * share

    small_copies[6].wait()
    for b in range(seq_rows):
        pair = cumul[b]
        cum_rows[b : b + 1, :] = pair[0:1, :]
        cum_rows[pad + b : pad + b + 1, :] = pair[1:2, :]
    seq_lane = lax.broadcasted_iota(jnp.int32, (1, seq_rows), 1)
    counts = lengths[...].astype(f32)
    limit = jnp.sum(jnp.where(seq_lane == row_seq, counts, 0.0), axis=-1, keepdims=True)
    limit = limit.astype(jnp.int32)
    position = lax.broadcasted_iota(jnp.int32, (1, span), 1)
    cum = cum_rows[...]
    last = jnp.sum(jnp.where(position == limit - 1, cum, 0.0), axis=-1, keepdims=True)
    scores = jnp.where(position < limit, scores + (last - cum) + log_forget, -jnp.inf)
    top = jnp.maximum(jnp.max(scores, axis=-1, keepdims=True), own)
    expo = jnp.exp(scores - top)
    own_exp = jnp.exp(own - top)
    total = jnp.sum(expo, axis=-1, keepdims=True) + own_exp
    weights = (expo / total).astype(bf16)
    own_weight = (own_exp / total).astype(bf16).astype(f32)

    folded = jnp.zeros((2 * pad, 2 * HD), f32)
    for i, r in enumerate(starts):
        size = min(chunk, total_rows - r)
        value_copies[i].wait()
        wide = lax.dot_general(
            weights, value_buf[r : r + size, :], nt, preferred_element_type=f32
        )
        seq = lax.broadcasted_iota(jnp.int32, (1, size), 1) // HD + r // HD
        wide = jnp.where(seq == row_seq, wide, 0.0)
        for c in range(0, size, 2 * HD):
            piece = wide[:, c : min(c + 2 * HD, size)]
            if piece.shape[1] < 2 * HD:
                piece = jnp.concatenate([piece, jnp.zeros_like(piece)], axis=1)
            folded = folded + piece
    mixed = folded + pltpu.roll(folded, HD, 1)
    mixed = mixed + own_weight * jnp.concatenate(
        [jnp.concatenate([new_values, new_values], axis=1)] * 2, axis=0
    )
    heads = jnp.where(low, mixed[0:pad, :], mixed[pad : 2 * pad, :]).astype(bf16)
    small_copies[7].wait()
    partial = jnp.dot(heads, wo[...], preferred_element_type=f32).astype(bf16)
    for n in range(out.shape[0]):
        out[n] = partial[0:seq_rows, :]
    for copy in pack_loads:
        copy.wait()


def attention_call(
    tokens,
    gain,
    wq,
    wk,
    wv,
    wf,
    bias,
    wo,
    keys,
    values,
    cumul,
    lengths,
    wg,
    wu,
    wd,
    routes,
    shares,
    blocks,
    slots,
    capacity,
):
    seq_rows, width = tokens.shape
    span = keys.shape[3]
    pad = 16
    chunk = 2 * HD * -(-seq_rows // 2)
    count = -(-seq_rows * HD // chunk)
    vmem = pl.BlockSpec(memory_space=pltpu.VMEM)
    hbm = pl.BlockSpec(memory_space=pl.ANY)
    kernel = functools.partial(attention_kernel, seq_rows=seq_rows, pad=pad, chunk=chunk, capacity=capacity)
    return pl.pallas_call(
        kernel,
        out_shape=(
            pltpu.VMEM((blocks, seq_rows, width), jnp.bfloat16),
            pltpu.VMEM((3,) + wg.shape, jnp.bfloat16),
            pltpu.VMEM((slots, seq_rows), jnp.bfloat16),
            pltpu.VMEM((slots, seq_rows), jnp.float32),
        ),
        in_specs=[hbm] * 17,
        out_specs=(vmem, vmem, vmem, vmem),
        scratch_shapes=[
            pltpu.VMEM(routes.shape, jnp.int32),
            pltpu.VMEM(shares.shape, jnp.float32),
            pltpu.VMEM((1, seq_rows), jnp.int32),
            pltpu.VMEM((1, bias.shape[0]), jnp.float32),
            pltpu.VMEM(tokens.shape, jnp.bfloat16),
            pltpu.VMEM((1, width), jnp.float32),
            pltpu.VMEM(wq.shape, jnp.bfloat16),
            pltpu.VMEM((HD, width), jnp.bfloat16),
            pltpu.VMEM((HD, width), jnp.bfloat16),
            pltpu.VMEM((2, width), jnp.bfloat16),
            pltpu.VMEM(wo.shape, jnp.bfloat16),
            pltpu.VMEM(cumul.shape, jnp.float32),
            pltpu.VMEM((seq_rows * HD, span), jnp.bfloat16),
            pltpu.VMEM((seq_rows * HD, span), jnp.bfloat16),
            pltpu.VMEM((2 * pad, span), jnp.float32),
            pltpu.VMEM((pad, width), jnp.float32),
            pltpu.SemaphoreType.DMA((12,)),
            pltpu.SemaphoreType.DMA((count,)),
            pltpu.SemaphoreType.DMA((count,)),
            pltpu.SemaphoreType.DMA((2 + width // wg.shape[1],)),
        ],
        name="attention",
    )(
        lengths.reshape(1, seq_rows),
        bias.reshape(1, -1),
        tokens,
        gain.reshape(1, width),
        wq,
        wk.T,
        wv.T,
        wf.T,
        wo,
        cumul,
        keys.reshape(seq_rows * HD, span),
        values.reshape(seq_rows * HD, span),
        wg,
        wu,
        wd,
        routes,
        shares,
    )


def expert_kernel(rows, trio, far, out, far_buf, far_sems, *, blocks):
    copies = [
        pltpu.make_async_copy(far.at[i], far_buf.at[i], far_sems.at[i]) for i in range(3)
    ]
    for copy in copies:
        copy.start()
    f32 = jnp.float32
    bf16 = jnp.bfloat16
    count, width = rows.shape
    cols = width // blocks
    units = trio.shape[2]
    capacity = out.shape[1]
    flats = [rows[:, n * cols : (n + 1) * cols] for n in range(blocks)]

    def matrix(pack, i, span):
        if pack == 3:
            return far_buf[i, span, :]
        return trio[3 * pack + i, span, :]

    def projected(pair, i):
        total = 0.0
        for n in range(blocks):
            span = slice(n * cols, (n + 1) * cols)
            weight = jnp.concatenate([matrix(pack, i, span) for pack in pair], axis=1)
            total = total + jnp.dot(flats[n], weight, preferred_element_type=f32)
        return total

    pairs = [(0, 1), (2, 3)]
    hiddens = []
    for pair in pairs:
        if pair[1] == 3:
            for copy in copies:
                copy.wait()
        gate = projected(pair, 0)
        up = projected(pair, 1)
        hiddens.append((gate / (1.0 + jnp.exp(-gate)) * up).astype(bf16))
    for n in range(blocks):
        part = 0.0
        for pair, hidden in zip(pairs, hiddens):
            strips = []
            for j in range(n * cols // units, (n + 1) * cols // units):
                span = slice(j * units, (j + 1) * units)
                strips.append(jnp.concatenate([matrix(pack, 2, span) for pack in pair], axis=0))
            weight = jnp.concatenate(strips, axis=1)
            part = part + jnp.dot(hidden, weight, preferred_element_type=f32)
        slots = count // capacity
        for e in range(slots):
            out[e * blocks + n] = part[e * capacity : (e + 1) * capacity, :].astype(bf16)


def expert_call(rows, trio, far, blocks, capacity):
    vmem = pl.BlockSpec(memory_space=pltpu.VMEM)
    hbm = pl.BlockSpec(memory_space=pl.ANY)
    count, width = rows.shape
    return pl.pallas_call(
        functools.partial(expert_kernel, blocks=blocks),
        out_shape=pltpu.VMEM(
            (blocks * count // capacity, capacity, width // blocks), jnp.bfloat16
        ),
        in_specs=[vmem, vmem, hbm],
        out_specs=vmem,
        scratch_shapes=[
            pltpu.VMEM(far.shape, jnp.bfloat16),
            pltpu.SemaphoreType.DMA((3,)),
        ],
        name="expert",
    )(in_vmem(rows), in_vmem(trio), far)


def outgoing_kernel(partials, tokens, gain, place, out, kept):
    f32 = jnp.float32
    bf16 = jnp.bfloat16
    mixed = sum(partials[n].astype(f32) for n in range(partials.shape[0]))
    residual = (tokens[...].astype(f32) + mixed).astype(bf16)
    kept[...] = residual
    rows = residual.astype(f32)
    inv = lax.rsqrt(jnp.sum(rows * rows, axis=-1, keepdims=True) / rows.shape[1] + EPSILON)
    ffn_in = (rows * inv * gain[...]).astype(bf16)
    spread = jnp.dot(place[...], ffn_in, preferred_element_type=f32)
    capacity = out.shape[1]
    for e in range(out.shape[0]):
        out[e] = spread[e * capacity : (e + 1) * capacity, :].astype(bf16)


def outgoing_call(partials, tokens, gain, place, capacity):
    vmem = pl.BlockSpec(memory_space=pltpu.VMEM)
    _, seq_rows, width = partials.shape
    return pl.pallas_call(
        outgoing_kernel,
        out_shape=(
            pltpu.VMEM((place.shape[0] // capacity, capacity, width), jnp.bfloat16),
            pltpu.VMEM((seq_rows, width), jnp.bfloat16),
        ),
        in_specs=[vmem] * 4,
        out_specs=(vmem, vmem),
        name="outgoing",
    )(in_vmem(partials), in_vmem(tokens), in_vmem(gain.reshape(1, -1)), in_vmem(place))


def in_vmem(array):
    return pltpu.with_memory_space_constraint(array, pltpu.VMEM)


def body(
    tokens,
    attn_gain,
    query_weight,
    key_weight,
    value_weight,
    forget_weight,
    forget_bias,
    out_weight,
    key_cache,
    value_cache,
    cum_forget,
    lengths,
    ffn_gain,
    routes,
    route_weights,
    gate_weight,
    up_weight,
    down_weight,
):
    tp_count = lax.axis_size("tp")
    ep_count = lax.axis_size(EXPERT_AXES) * SLICES
    tp_rank = lax.axis_index("tp")
    seq_rows = tokens.shape[0]
    width = tokens.shape[1]
    cols = width // tp_count
    experts = ep_count // SLICES
    capacity = min(seq_rows, max(2, (2 * seq_rows * TOP_K + experts - 1) // experts))
    partial, own_pack, place, weighted = attention_call(
        tokens,
        attn_gain,
        query_weight,
        key_weight,
        value_weight,
        forget_weight,
        forget_bias,
        out_weight,
        key_cache,
        value_cache,
        cum_forget,
        lengths,
        gate_weight[0],
        up_weight[0],
        down_weight[0],
        routes.T,
        route_weights.T,
        tp_count,
        experts * capacity,
        capacity,
    )
    blocks = lax.all_to_all(partial, "tp", 0, 0, tiled=True)
    swap = [(0, 1), (1, 0)]
    side_pack = lax.ppermute(own_pack, "xl", swap)
    core_pack = lax.ppermute(own_pack, "core", swap)
    far_pack = lax.ppermute(side_pack, "core", swap)
    trio = jnp.concatenate([own_pack, core_pack, side_pack], axis=0)
    outgoing, residual = outgoing_call(blocks, tokens, ffn_gain, place, capacity)
    arrived = lax.all_to_all(outgoing, EXPERT_AXES, split_axis=0, concat_axis=0, tiled=True)
    arrived = arrived.reshape(experts * capacity, width)
    residual_cols = lax.dynamic_slice_in_dim(residual, tp_rank * cols, cols, 1)
    part = expert_call(arrived, trio, far_pack, tp_count, capacity)
    part, residual_cols = lax.optimization_barrier((part, residual_cols))
    parts = lax.all_to_all(part, EXPERT_AXES + ("tp",), split_axis=0, concat_axis=0, tiled=True)
    parts = parts.reshape(experts, tp_count, capacity, cols)
    returned = jnp.sum(parts.astype(jnp.float32), axis=1).reshape(experts * capacity, cols)
    routed = lax.dot_general(
        weighted,
        returned,
        (((0,), (0,)), ((), ())),
        precision=lax.Precision.HIGHEST,
        preferred_element_type=jnp.float32,
    )
    return (residual_cols.astype(jnp.float32) + routed).astype(jnp.bfloat16)


def solution(mesh):
    half = mesh.shape["ep"] // (2 * SLICES)
    fine = Mesh(
        mesh.devices.reshape(half, 2, 2, 2, mesh.shape["tp"]), EP_AXES + ("tp",)
    )
    return jax.shard_map(
        body,
        mesh=fine,
        in_specs=(
            P(EP_AXES, None),
            P(),
            P(None, "tp"),
            P(None, "tp"),
            P(None, "tp"),
            P(None, "tp"),
            P("tp"),
            P("tp", None),
            P(EP_AXES, "tp", None, None),
            P(EP_AXES, "tp", None, None),
            P(EP_AXES, "tp", None),
            P(EP_AXES),
            P(),
            P(EP_AXES, None),
            P(EP_AXES, None),
            P(EP_AXES, None, "tp"),
            P(EP_AXES, None, "tp"),
            P(EP_AXES, "tp", None),
        ),
        out_specs=P(EP_AXES, "tp"),
        check_vma=False,
    )
```
